32 devices in a mesh: rep: 2 (over x), fs: 8 (over z, y), tp: 2 (over core).
Axes of the slice: x: 2, y: 2, z: 4, core: 2. Of those that a mesh axis runs over, the one named last changes fastest.
Arguments:
- stream_in: bfloat16 [16, 1024, 2048], P(('rep', 'fs'), None, 'tp'), may hold values from -48 to 48
- decay_shift: float32 [16, 1024], P(('rep', 'fs')), may hold values from -1.5 to 0, as said below
- mixer_gain: float32 [2048], replicated, may hold values from 0.1 to 1.9
- gate_weight: bfloat16 [2048, 1024], P('fs', 'tp'), may hold values from -0.125 to 0.125
- input_weight: bfloat16 [2048, 1024], P('fs', 'tp'), may hold values from -0.125 to 0.125
- filter_taps: float32 [4, 1024], P(None, 'tp'), may hold values from -3 to 3
- recur_gate: bfloat16 [4, 256, 256], P('tp'), may hold values from -0.375 to 0.375
- inlet_gate: bfloat16 [4, 256, 256], P('tp'), may hold values from -0.375 to 0.375
- decay_param: float32 [1024], P('tp'), may hold values from 1.5 to 12
- mixer_out: bfloat16 [1024, 2048], P('tp', 'fs'), may hold values from -0.1875 to 0.1875
- feedforward_gain: float32 [2048], replicated, may hold values from 0.1 to 1.9
- up_weight: bfloat16 [2048, 4096], P('fs', 'tp'), may hold values from -0.125 to 0.125
- down_weight: bfloat16 [4096, 2048], P('tp', 'fs'), may hold values from -0.09375 to 0.09375
- final_gain: float32 [2048], P('tp'), may hold values from 0.1 to 1.9
Outputs:
- layer_out: bfloat16 [16, 1024, 2048], P(('rep', 'fs'), None, 'tp')
The draws below stay inside these ranges and needn't reach their ends.
Inputs may be any that keep to these rules, and one draw needn't show every extreme that they name: `decay_shift`: every entry is negative.
All inputs are finite; a program needn't handle non-finite values.
Results may differ from the reference program's by a relative error of at most 0.015.
Values may be sent and summed in bfloat16 or wider, within the bound.
A program may use at most 128 MiB of HBM per device.

```python
import math
import jax
import jax.numpy as jnp
from jax import lax

D = 2048
NB = 4
BLOCK = 256
DR = 1024
FF = 4096
TAPS = 4
LENGTH = 1024
SEQS = 16
N_TP = 2


def draw_stream_in(key, part):
    starting_level = jax.random.normal(jax.random.fold_in(key, 1), (SEQS, LENGTH, D), jnp.float32)
    ramp = jnp.exp(jnp.linspace(math.log(0.5), math.log(2.0), D)).astype(jnp.float32)
    lower, upper = (math.log(0.5), math.log(2.0))
    row_scale = jnp.exp(jax.random.uniform(jax.random.fold_in(key, 2), (SEQS, LENGTH, 1), jnp.float32, lower, upper))
    return (jnp.clip(starting_level, -6.0, 6.0) * ramp[None, None, :] * row_scale).astype(jnp.bfloat16)


def draw_decay_param(key, part):
    fast_cut = 5
    fast = jax.random.randint(jax.random.fold_in(key, 11), (DR,), 0, 10) < fast_cut
    keep = jnp.exp(jax.random.uniform(jax.random.fold_in(key, 12), (DR,), jnp.float32, math.log(0.4), math.log(0.9)))
    slow_rate = -jnp.log(keep) / LENGTH
    short_span = float(min(30, LENGTH // 4))
    long_span = float(min(100, LENGTH // 2))
    fast_rate = 2.3 / jax.random.uniform(jax.random.fold_in(key, 13), (DR,), jnp.float32, short_span, long_span)
    rate = jnp.where(fast, fast_rate, slow_rate) / (8.0 * 0.5)
    return (-jnp.log(jnp.expm1(rate))).astype(jnp.float32)


def draw_decay_shift(key, part):
    starting_level = -jnp.exp(jax.random.uniform(jax.random.fold_in(key, 21), (SEQS, 1), jnp.float32, math.log(0.105), math.log(0.69))) / LENGTH
    spots = jax.random.randint(jax.random.fold_in(key, 22), (SEQS, 2), 0, LENGTH)
    number_of_tiers = jnp.log(jax.random.uniform(jax.random.fold_in(key, 23), (SEQS, 2), jnp.float32, 0.5, 0.8))
    places = jnp.arange(LENGTH, dtype=jnp.int32)
    agreement_tally = (places[None, None, :] == spots[:, :, None]).astype(jnp.float32)
    spike_source = jnp.sum(agreement_tally * number_of_tiers[:, :, None], axis=1)
    return (starting_level + spike_source).astype(jnp.float32)


def block_scale(own_key, dims, split, smallest, high):
    gain, own = 1.0, jax.random.fold_in(own_key, 6)
    for axis_at, shards_of in split:
        steps = jnp.exp(jax.random.uniform(jax.random.fold_in(own, axis_at), (shards_of,), jnp.float32, smallest / len(split), high / len(split)))
        gain = gain * jnp.repeat(steps, dims[axis_at] // shards_of).reshape([-1 if axis == axis_at else 1 for axis in range(len(dims))])
    return gain


def normal_values(own_key, shape, width, bound, split=(), kind=jnp.bfloat16):
    entries = width * jax.random.normal(own_key, shape, jnp.float32)
    if split:
        entries = entries * block_scale(own_key, shape, split, -0.22, 0.18)
    return jnp.clip(entries, -bound, bound).astype(kind)


def setup_inputs(seed: int = 0) -> dict:
    key_of = jax.random.split(jax.random.key(seed), 15)
    return {
        "stream_in": draw_stream_in(jax.random.fold_in(key_of[14], 71), 0),
        "decay_shift": draw_decay_shift(jax.random.fold_in(key_of[14], 71), 0),
        "mixer_gain": jnp.clip(1.0 + 0.18 * jax.random.normal(key_of[2], (D,), jnp.float32), 0.1, 1.9),
        "gate_weight": normal_values(key_of[3], (D, DR), D ** -0.5, 0.125, ((0, 8), (1, 2))),
        "input_weight": normal_values(key_of[4], (D, DR), D ** -0.5, 0.125, ((0, 8), (1, 2))),
        "filter_taps": normal_values(key_of[5], (TAPS, DR), 0.5, 3.0, ((1, 2),), jnp.float32),
        "recur_gate": normal_values(key_of[6], (NB, BLOCK, BLOCK), BLOCK ** -0.5, 0.375, ((0, 2),)),
        "inlet_gate": normal_values(key_of[7], (NB, BLOCK, BLOCK), BLOCK ** -0.5, 0.375, ((0, 2),)),
        "decay_param": draw_decay_param(jax.random.fold_in(key_of[14], 71), 0),
        "mixer_out": normal_values(key_of[9], (DR, D), DR ** -0.5, 0.1875, ((0, 2), (1, 8))),
        "feedforward_gain": jnp.clip(1.0 + 0.18 * jax.random.normal(key_of[10], (D,), jnp.float32), 0.1, 1.9),
        "up_weight": normal_values(key_of[11], (D, FF), D ** -0.5, 0.125, ((0, 8), (1, 2))),
        "down_weight": normal_values(key_of[12], (FF, D), FF ** -0.5, 0.09375, ((0, 2), (1, 8))),
        "final_gain": jnp.clip(1.0 + 0.18 * jax.random.normal(key_of[13], (D,), jnp.float32), 0.1, 1.9),
    }


epsilon = 1e-06
rate_scale = 8.0

def norm_rows(values, row_gain):
    mean_sq = lax.optimization_barrier(jnp.mean(values * values, axis=-1, keepdims=True))
    return values * lax.rsqrt(mean_sq + epsilon) * row_gain

def split_sum(left, right):
    share = right.shape[0] // N_TP
    total = jnp.zeros((left.shape[0], right.shape[1]), jnp.float32)
    for index in range(N_TP):
        partial_prod = jnp.dot(left[:, index * share:(index + 1) * share], right[index * share:(index + 1) * share], preferred_element_type=jnp.float32)
        rounded = lax.optimization_barrier(partial_prod.astype(jnp.bfloat16))
        total = total + rounded.astype(jnp.float32)
    return total

def combine(earlier, later):
    return (earlier[0] * later[0], later[0] * earlier[1] + later[1])

def reference(stream_in, decay_shift, mixer_gain, gate_weight, input_weight, filter_taps, recur_gate, inlet_gate, decay_param, mixer_out, feedforward_gain, up_weight, down_weight, final_gain):

    def one_sequence(inputs):
        seq_in, shift_row = inputs
        length = seq_in.shape[0]
        stream_f = seq_in.astype(jnp.float32)
        normed = norm_rows(stream_f, mixer_gain).astype(jnp.bfloat16)
        gate_logits = jnp.dot(normed, gate_weight, preferred_element_type=jnp.float32).astype(jnp.bfloat16)
        input_pre = jnp.dot(normed, input_weight, preferred_element_type=jnp.float32).astype(jnp.bfloat16)
        branch = jax.nn.gelu(gate_logits.astype(jnp.float32), approximate=True)
        extended_front = jnp.pad(input_pre.astype(jnp.float32), ((TAPS - 1, 0), (0, 0)))
        filtered = jnp.zeros(input_pre.shape, jnp.float32)
        for offset in range(TAPS):
            filtered = filtered + extended_front[offset:offset + length] * filter_taps[offset][None, :]
        filtered = filtered.astype(jnp.bfloat16)
        grouped = filtered.astype(jnp.float32).reshape(length, NB, BLOCK)
        recur = jax.nn.sigmoid(jnp.einsum('lni,nij->lnj', grouped, recur_gate.astype(jnp.float32)).reshape(length, DR))
        inlet = jax.nn.sigmoid(jnp.einsum('lni,nij->lnj', grouped, inlet_gate.astype(jnp.float32)).reshape(length, DR))
        logarithm_decay = -rate_scale * recur * jax.nn.softplus(-decay_param)[None, :] + shift_row[:, None]
        decay = jnp.exp(logarithm_decay)
        drive = jnp.sqrt(-jnp.expm1(2.0 * logarithm_decay)) * inlet * filtered.astype(jnp.float32)
        states = lax.associative_scan(combine, (decay, drive), axis=0)[1]
        mixed = (states * branch).astype(jnp.bfloat16)
        mixer_sum = split_sum(mixed, mixer_out)
        stream_mid = (stream_f + mixer_sum).astype(jnp.bfloat16)
        normed_mid = norm_rows(stream_mid.astype(jnp.float32), feedforward_gain).astype(jnp.bfloat16)
        up_proj = jnp.dot(normed_mid, up_weight, preferred_element_type=jnp.float32)
        activated = jnp.square(jax.nn.relu(up_proj)).astype(jnp.bfloat16)
        ffn_sum = split_sum(activated, down_weight)
        total = stream_mid.astype(jnp.float32) + ffn_sum
        return norm_rows(total, final_gain).astype(jnp.bfloat16)
    return lax.map(one_sequence, (stream_in, decay_shift))
```

```python
import functools

import jax
import jax.numpy as jnp
from jax import lax
from jax.experimental import pallas as pl
from jax.experimental.pallas import tpu as pltpu
from jax.sharding import PartitionSpec as P

D = 2048


epsilon = 1e-06
rate_scale = 8.0


def norm_rows(values, row_gain):
    mean_sq = jnp.mean(values * values, axis=-1, keepdims=True)
    return values * lax.rsqrt(mean_sq + epsilon) * row_gain


def combine(earlier, later):
    return (earlier[0] * later[0], later[0] * earlier[1] + later[1])


def plain(
    stream_in,
    decay_shift,
    mixer_gain,
    gate_weight,
    input_weight,
    filter_taps,
    recur_gate,
    inlet_gate,
    decay_param,
    mixer_out,
    feedforward_gain,
    up_weight,
    down_weight,
    final_gain,
):
    num_seq, length, half_width = stream_in.shape
    whole = lax.all_gather(stream_in, "tp", axis=2, tiled=True)
    flat_rows = num_seq * length
    normed = norm_rows(whole.reshape(flat_rows, -1).astype(jnp.float32), mixer_gain).astype(
        jnp.bfloat16
    )
    channels = gate_weight.shape[1]
    columns = normed
    gate_logits = jnp.dot(
        columns,
        lax.all_gather(gate_weight, "fs", axis=0, tiled=True),
        preferred_element_type=jnp.float32,
    )
    input_pre = jnp.dot(
        columns,
        lax.all_gather(input_weight, "fs", axis=0, tiled=True),
        preferred_element_type=jnp.float32,
    )
    gate_logits = gate_logits.astype(jnp.bfloat16)
    input_pre = input_pre.astype(jnp.bfloat16)
    branch = jax.nn.gelu(gate_logits.astype(jnp.float32), approximate=True)
    num_taps = filter_taps.shape[0]
    extended_front = jnp.pad(
        input_pre.astype(jnp.float32).reshape(num_seq, length, channels),
        ((0, 0), (num_taps - 1, 0), (0, 0)),
    )
    filtered = jnp.zeros((num_seq, length, channels), jnp.float32)
    for offset in range(num_taps):
        filtered = (
            filtered
            + extended_front[:, offset : offset + length] * filter_taps[offset][None, None, :]
        )
    filtered = filtered.astype(jnp.bfloat16).reshape(flat_rows, channels)
    num_blocks = recur_gate.shape[0]
    grouped = filtered.reshape(flat_rows, num_blocks, recur_gate.shape[1])
    recur = jax.nn.sigmoid(
        jnp.einsum("lni,nij->lnj", grouped, recur_gate, preferred_element_type=jnp.float32).reshape(
            flat_rows, channels
        )
    )
    inlet = jax.nn.sigmoid(
        jnp.einsum("lni,nij->lnj", grouped, inlet_gate, preferred_element_type=jnp.float32).reshape(
            flat_rows, channels
        )
    )
    logarithm_decay = (
        -rate_scale * recur * jax.nn.softplus(-decay_param)[None, :]
        + decay_shift.reshape(flat_rows)[:, None]
    )
    decay = jnp.exp(logarithm_decay).reshape(num_seq, length, channels)
    drive = (
        jnp.sqrt(-jnp.expm1(2.0 * logarithm_decay)) * inlet * filtered.astype(jnp.float32)
    ).reshape(num_seq, length, channels)
    states = lax.associative_scan(combine, (decay, drive), axis=1)[1]
    mixed = (states.reshape(flat_rows, channels) * branch).astype(jnp.bfloat16)
    mixer_terms = (
        jnp.dot(
            mixed,
            lax.all_gather(mixer_out, "fs", axis=1, tiled=True),
            preferred_element_type=jnp.float32,
        )
        .astype(jnp.bfloat16)
        .astype(jnp.float32)
    )
    mixer_sum = lax.psum_scatter(
        mixer_terms.astype(jnp.bfloat16), "tp", scatter_dimension=1, tiled=True
    ).astype(jnp.float32)
    stream_mid = (stream_in.reshape(flat_rows, half_width).astype(jnp.float32) + mixer_sum).astype(
        jnp.bfloat16
    )
    stream_whole = lax.all_gather(stream_mid, "tp", axis=1, tiled=True)
    normed_mid = norm_rows(stream_whole.astype(jnp.float32), feedforward_gain).astype(jnp.bfloat16)
    columns = normed_mid
    up_proj = jnp.dot(
        columns,
        lax.all_gather(up_weight, "fs", axis=0, tiled=True),
        preferred_element_type=jnp.float32,
    )
    activated = jnp.square(jax.nn.relu(up_proj)).astype(jnp.bfloat16)
    ffn_terms = (
        jnp.dot(
            activated,
            lax.all_gather(down_weight, "fs", axis=1, tiled=True),
            preferred_element_type=jnp.float32,
        )
        .astype(jnp.bfloat16)
        .astype(jnp.float32)
    )
    ffn_sum = lax.psum_scatter(
        ffn_terms.astype(jnp.bfloat16), "tp", scatter_dimension=1, tiled=True
    ).astype(jnp.float32)
    total = stream_mid.astype(jnp.float32) + ffn_sum
    squares_sum = lax.psum(jnp.sum(total * total, axis=1), "tp")
    layer_out = total * lax.rsqrt(squares_sum / D + epsilon)[:, None] * final_gain[None, :]
    return layer_out.astype(jnp.bfloat16).reshape(num_seq, length, half_width)


F32 = jnp.float32
BF16 = jnp.bfloat16
TILE = 16
FORE, BACK, BOTH = range(3)
ROWS = 256


def split_rows(rows, up):
    third = rows // 3 // TILE * TILE + (TILE if up else 0)
    return rows - 2 * third, third


def expm1_neg(v):
    series = -v * (1.0 + v * (1 / 2) * (1.0 + v * (1 / 3) * (1.0 + v * (1 / 4) * (1.0 + v * (1 / 5) * (1.0 + v * (1 / 6))))))
    return jnp.where(v > -0.25, series, 1.0 - jnp.exp(v))


def layer_kernel(
    n,
    x_in, shift_ref, mgain_ref, wg_in, wi_in, taps_ref, rg_ref, ig_ref, sp_ref, wo_in,
    fgain_ref, wu_in, wd_in,
    out_ref, scale_ref,
    x_ref, wg, wi, wo, wu, wd, other, normed, front, carry, scan_a, scan_b, part, prec, mid, mid_other,
    act, sq_send, sq_recv,
    local_sems, send_sems, recv_sems, tp_send, tp_recv, out_sems,
):
    rep, fs, tp = lax.axis_index("rep"), lax.axis_index("fs"), lax.axis_index("tp")
    half_n = n // 2
    length, half = x_in.shape
    channels = wg.shape[1]
    width = wd.shape[2]
    shard = wg_in.shape[0]
    hidden = wu.shape[1]
    blocks = length // ROWS

    def ring_to_fs(p):
        p = lax.rem(p + 2 * n, n)
        return jnp.where(p < half_n, 2 * p, 2 * (n - 1 - p) + 1)

    odd = lax.rem(fs, 2)
    pos = (1 - odd) * (fs // 2) + odd * (n - 1 - fs // 2)
    right, left = ring_to_fs(pos + 1), ring_to_fs(pos - 1)

    def by_row(dst, lo, cols):
        def view(owner, off, size):
            return dst.at[pl.ds(pl.multiple_of(owner * shard + off, TILE), size), pl.ds(lo, cols)]
        return view

    def by_owner(dst, lo):
        def view(owner, off, size):
            return dst.at[owner, pl.ds(pl.multiple_of(lo + off, TILE), size), :]
        return view

    rows_o, rows_d = wo.shape[1], wd.shape[1]
    cut = hidden * 3 // 8
    rest = (hidden - cut) // 2
    last = rows_d // 16
    main = (rows_d - 2 * last) // 2
    views = [
        (by_row(wg, 0, channels), BACK, split_rows(shard, True)),
        (by_row(wi, 0, channels), FORE, split_rows(shard, True)),
        (by_owner(wo, 0), FORE, split_rows(rows_o, False)),
        (by_row(wu, 0, cut), BACK, split_rows(shard, True)),
        (by_row(wu, cut, rest), FORE, split_rows(shard, True)),
        (by_row(wu, cut + rest, rest), BACK, split_rows(shard, False)),
        (by_owner(wd, 0), FORE, split_rows(main, False)),
        (by_owner(wd, main), BACK, split_rows(main, False)),
        (by_owner(wd, 2 * main), BOTH, (last, last)),
    ]
    ups = range(3, 6)
    downs = range(6, 9)

    def remote(view, k, lane, s, device):
        return pltpu.make_async_remote_copy(
            src_ref=view, dst_ref=view, send_sem=send_sems.at[k, lane, s],
            recv_sem=recv_sems.at[k, lane, s], device_id=device,
            device_id_type=pl.DeviceIdType.MESH,
        )

    def cw(k, s, shift=0):
        view, role, (p, q) = views[k]
        lo, size = (p + rep * q, q) if role == BACK else (0, p)
        return remote(view(ring_to_fs(pos - s - shift), lo, size), k, 0, s, {"fs": right})

    def ccw(k, s, shift=0):
        view, role, (p, q) = views[k]
        lo, size = (p + rep * q, q) if role == FORE else (p if role == BOTH else 0, q if role == BOTH else p)
        return remote(view(ring_to_fs(pos + s + shift), lo, size), k, 1, s, {"fs": left})

    def across(k, s, side):
        view, role, (p, q) = views[k]
        owner = pos + s + 1 if role == FORE else pos - s - 1
        return remote(view(ring_to_fs(owner), p + side * q, q), k, 2, s, {"rep": 1 - rep})

    def shared(k):
        return views[k][1] != BOTH

    def begin(k):
        cw(k, 0).start()
        ccw(k, 0).start()

    def service(k, s, last):
        def forward(make):
            if last is None:
                pl.when(s + 1 < n - 1)(lambda: make(k, s + 1).start())
            elif not last:
                make(k, s + 1).start()

        cw(k, s, 1).wait_recv()
        forward(cw)
        if views[k][1] == BACK:
            across(k, s, rep).start()
        ccw(k, s, 1).wait_recv()
        forward(ccw)
        if views[k][1] == FORE:
            across(k, s, rep).start()

    def wait_across(k, s):
        if shared(k):
            across(k, s, 1 - rep).wait_recv()

    def swap(src, dst, index):
        return pltpu.make_async_remote_copy(
            src_ref=src, dst_ref=dst, send_sem=tp_send.at[index], recv_sem=tp_recv.at[index],
            device_id={"tp": 1 - tp}, device_id_type=pl.DeviceIdType.MESH,
        )

    own = [
        (x_in, x_ref),
        (wg_in, wg.at[pl.ds(pl.multiple_of(fs * shard, TILE), shard), :]),
        (wi_in, wi.at[pl.ds(pl.multiple_of(fs * shard, TILE), shard), :]),
        (wo_in, wo.at[fs]),
        (wu_in, wu.at[pl.ds(pl.multiple_of(fs * shard, TILE), shard), :]),
        (wd_in, wd.at[fs]),
    ]
    local = [pltpu.make_async_copy(a, b, local_sems.at[i]) for i, (a, b) in enumerate(own)]
    for i in (1, 2, 3, 0, 4, 5):
        local[i].start()
    barrier = pltpu.get_barrier_semaphore()
    for device in ({"fs": right}, {"fs": left}, {"rep": 1 - rep}, {"tp": 1 - tp}):
        pl.semaphore_signal(barrier, inc=1, device_id=device, device_id_type=pl.DeviceIdType.MESH)
    pl.semaphore_wait(barrier, 4)
    swap_x = swap(x_ref, other, 0)
    for k in range(3):
        local[1 + k].wait()
        begin(k)
    local[0].wait()
    swap_x.start()
    local[4].wait()
    local[5].wait()

    own_cols = pl.ds(pl.multiple_of(tp * half, 128), half)
    other_cols = pl.ds(pl.multiple_of((1 - tp) * half, 128), half)

    def norm_block(first, second, gain_ref, rows):
        a = first[rows, :].astype(F32)
        b = second[rows, :].astype(F32)
        mean = (jnp.sum(a * a, axis=1, keepdims=True) + jnp.sum(b * b, axis=1, keepdims=True)) / (2 * half)
        scale = lax.rsqrt(mean + epsilon)
        normed[rows, own_cols] = (a * scale * gain_ref[:, own_cols]).astype(BF16)
        normed[rows, other_cols] = (b * scale * gain_ref[:, other_cols]).astype(BF16)

    small = 64

    pieces = length // small
    share = -(-pieces // (n - 2))

    @pl.loop(0, n - 2)
    def _(s):
        for k in range(3):
            service(k, s, False)
        pl.when(s == 0)(swap_x.wait)
        for k in list(ups)[:2]:
            pl.when(s == n - 3)(functools.partial(begin, k))
        for piece in range(share):
            i = s * share + piece

            @pl.when(i < pieces)
            def _():
                norm_block(x_ref, other, mgain_ref, pl.ds(pl.multiple_of(i * small, small), small))

    begin(ups[-1])
    for k in range(3):
        service(k, n - 2, True)

    lead = n - 2

    def tick(t, j):
        pl.when(t < n - 1)(lambda: service(ups[j], t, None))
        if j == 2:
            for e, k in enumerate(downs):
                pl.when(t == (n - 4 if e == 0 else n - 3))(functools.partial(begin, k))
        pl.when(t >= lead)(lambda: service(downs[j], t - lead, None))

    for j in range(3):
        tick(0, j)

    @pl.loop(0, n - 1)
    def _(s):
        for k in range(3):
            wait_across(k, s)

    front[pl.ds(0, 8), :] = jnp.zeros((8, channels), F32)
    carry[...] = jnp.zeros_like(carry)
    decay_param = sp_ref[...]
    rate = rate_scale * (jnp.maximum(-decay_param, 0.0) + jnp.log1p(jnp.exp(-jnp.abs(decay_param))))
    num_taps = taps_ref.shape[0]
    groups = rg_ref.shape[0]
    block = rg_ref.shape[1]
    @pl.loop(0, blocks)
    def _(i):
        rows = pl.ds(pl.multiple_of(i * ROWS, ROWS), ROWS)
        tick(i + 1, 0)
        cols = normed[rows, :]
        front[pl.ds(8, ROWS), :] = jnp.dot(cols, wi[...], preferred_element_type=F32).astype(BF16).astype(F32)
        gate = jnp.dot(cols, wg[...], preferred_element_type=F32).astype(BF16)
        shift = jnp.transpose(jnp.broadcast_to(shift_ref[:, rows], (128, ROWS)))[:, :1]
        for g in range(groups):
            if g == 1:
                tick(i + 1, 1)
            ch = slice(g * block, (g + 1) * block)
            window = front[:, ch]
            filtered = jnp.zeros((ROWS, block), F32)
            for tap in range(num_taps):
                back = num_taps - 1 - tap
                moved = window if back == 0 else pltpu.roll(window, back, 0)
                filtered = filtered + moved[8:] * taps_ref[tap : tap + 1, ch]
            filtered = filtered.astype(BF16)
            recur = jax.nn.sigmoid(jnp.dot(filtered, rg_ref[g], preferred_element_type=F32))
            inlet = jax.nn.sigmoid(jnp.dot(filtered, ig_ref[g], preferred_element_type=F32))
            log_decay = shift - recur * rate[:, ch]
            a = jnp.exp(log_decay)
            b = jnp.sqrt(expm1_neg(2.0 * log_decay)) * inlet * filtered.astype(F32)
            a = a.reshape(ROWS // 8, 8, block)
            b = b.reshape(ROWS // 8, 8, block)
            at = lax.broadcasted_iota(jnp.int32, (ROWS // 8, 8, block), 1)
            for back in (1, 2, 4):
                keep = at >= back
                b = jnp.where(keep, a * pltpu.roll(b, back, 1) + b, b)
                a = jnp.where(keep, a * pltpu.roll(a, back, 1), a)
            scan_a[:, ch] = a.reshape(ROWS, block)
            scan_b[:, ch] = b.reshape(ROWS, block)
        front[pl.ds(0, 8), :] = front[pl.ds(ROWS, 8), :]

        def step_scan(t, h):
            at = pl.ds(pl.multiple_of(t * 8, 8), 8)
            states = scan_a[at, :] * h + scan_b[at, :]
            scan_b[at, :] = states
            return jnp.broadcast_to(states[7:8, :], states.shape)

        carry[...] = lax.fori_loop(0, ROWS // 8, step_scan, carry[...], unroll=4)
        tick(i + 1, 2)
        mixed = (scan_b[...] * jax.nn.gelu(gate.astype(F32), approximate=True)).astype(BF16)
        for j in range(half_n):
            to = pl.ds(j * width, width)
            part[1, rows, to] = jnp.dot(mixed, wo[(1 - tp) * half_n + j], preferred_element_type=F32).astype(BF16)
        swap(part.at[1, rows, :], prec.at[rows, :], 1 + i).start()
        for j in range(half_n):
            to = pl.ds(j * width, width)
            part[0, rows, to] = jnp.dot(mixed, wo[tp * half_n + j], preferred_element_type=F32).astype(BF16)

    tick(blocks + 1, 0)

    @pl.loop(0, blocks)
    def _(i):
        rows = pl.ds(pl.multiple_of(i * ROWS, ROWS), ROWS)
        swap(part.at[1, rows, :], prec.at[rows, :], 1 + i).wait()
        mid[rows, :] = (
            x_ref[rows, :].astype(F32) + (part[0, rows, :].astype(F32) + prec[rows, :].astype(F32))
        ).astype(BF16)
        swap(mid.at[rows, :], mid_other.at[rows, :], 1 + blocks + i).start()

    tick(blocks + 1, 1)

    @pl.loop(0, blocks)
    def _(i):
        rows = pl.ds(pl.multiple_of(i * ROWS, ROWS), ROWS)
        swap(mid.at[rows, :], mid_other.at[rows, :], 1 + blocks + i).wait()

    tick(blocks + 1, 2)

    for part_of in range(2):

        @pl.loop(part_of * (pieces // 2), (part_of + 1) * (pieces // 2))
        def _(i):
            norm_block(mid, mid_other, fgain_ref, pl.ds(pl.multiple_of(i * small, small), small))

        tick(blocks + 2, part_of)

    tick(blocks + 2, 2)
    for t in range(blocks + 3, n):
        for j in range(3):
            tick(t, j)

    @pl.loop(0, n - 1)
    def _(s):
        for k in ups:
            wait_across(k, s)

    up_cols = min(512, hidden)
    @pl.loop(0, hidden // up_cols)
    def _(c):
        to = pl.ds(pl.multiple_of(c * up_cols, up_cols), up_cols)

        @pl.loop(0, blocks)
        def _(i):
            rows = pl.ds(pl.multiple_of(i * ROWS, ROWS), ROWS)
            up = jnp.maximum(jnp.dot(normed[rows, :], wu[:, to], preferred_element_type=F32), 0.0)
            act[rows, to] = (up * up).astype(BF16)

        for j in range(3):
            pl.when(c == j)(functools.partial(tick, n, j))

    tick(n + 1, 0)

    def place(owner, i):
        column = lax.rem(owner, half_n)
        slot = lax.rem(owner // half_n + tp, 2)
        rows = pl.ds(pl.multiple_of(i * ROWS, ROWS), ROWS)
        to = pl.ds(pl.multiple_of(column * width, 128), width)
        return column, slot, rows, to

    def back_swap(column, i):
        _, _, rows, to = place(column, i)
        return swap(part.at[1, rows, to], prec.at[rows, to], 1 + 2 * blocks + column * blocks + i)

    def write(column, i):
        _, _, rows, to = place(column, i)
        return pltpu.make_async_copy(other.at[rows, to], out_ref.at[rows, to], out_sems.at[column * blocks + i])

    def down_rows(owner, i):
        column, slot, rows, to = place(owner, i)
        part[slot, rows, to] = jnp.dot(act[rows, :], wd[owner], preferred_element_type=F32).astype(BF16)
        pl.when(slot == 1)(lambda: back_swap(column, i).start())

    def total_rows(owner, i):
        column, slot, rows, to = place(owner, i)

        @pl.when(slot == 0)
        def _():
            back_swap(column, i).wait_recv()
            total = mid[rows, to].astype(F32) + (part[0, rows, to].astype(F32) + prec[rows, to].astype(F32))
            other[rows, to] = total.astype(BF16)
            squares = total * total
            sq_send[rows, :] += sum(squares[:, at : at + 128] for at in range(0, width, 128))
            write(column, i).start()

    def over_rows(*makes):
        @pl.loop(0, blocks)
        def _(i):
            for make, owner in makes:
                make(owner, i)

    order = [ring_to_fs(pos + ahead) for ahead in [0, half_n]]
    for s in range(half_n, n - 1):
        order += [ring_to_fs(pos - s - 1), ring_to_fs(pos + s + 1)]
    sq_send[...] = jnp.zeros_like(sq_send)
    over_rows((down_rows, order[0]))
    for at in range(3 * n + 4, 3 * (lead + half_n + 1)):
        tick(at // 3, at % 3)
    for s in range(half_n - 1, n - 1):
        ahead = lead + s + 2
        for earlier in range(half_n) if s == half_n - 1 else [s]:
            for k in downs:
                wait_across(k, earlier)
        if s == half_n - 1:
            over_rows((down_rows, order[1]), (total_rows, order[0]))
        elif s < n - 2:
            at = 2 * (s - half_n + 1)
            over_rows((down_rows, order[at]), (total_rows, order[at - 1]))
            if s < n - 3:
                tick(ahead, 0)
            over_rows((down_rows, order[at + 1]), (total_rows, order[at]))
        if s < n - 3:
            for j in range(1 if s >= half_n else 0, 3):
                tick(ahead, j)
    over_rows((down_rows, order[-2]), (down_rows, order[-1]), (total_rows, order[-3]))

    def swap_sq(i):
        rows = pl.ds(pl.multiple_of(i * ROWS, ROWS), ROWS)
        return swap(sq_send.at[rows, :], sq_recv.at[rows, :], 1 + 2 * blocks + half_n * blocks + i)

    @pl.loop(0, blocks)
    def _(i):
        total_rows(order[-2], i)
        total_rows(order[-1], i)
        swap_sq(i).start()

    @pl.loop(0, blocks)
    def _(i):
        swap_sq(i).wait()
        rows = pl.ds(pl.multiple_of(i * ROWS, ROWS), ROWS)
        squares = jnp.sum(sq_send[rows, :] + sq_recv[rows, :], axis=1, keepdims=True)
        scale_ref[rows, :] = jnp.broadcast_to(lax.rsqrt(squares / (2 * half) + epsilon), (ROWS, 128))

    @pl.loop(0, n - 1)
    def _(s):
        for k in range(len(views)):
            cw(k, s).wait_send()
            ccw(k, s).wait_send()
            if shared(k):
                across(k, s, rep).wait_send()

    @pl.loop(0, blocks)
    def _(i):
        for j in range(half_n):
            back_swap(j, i).wait_send()
            write(j, i).wait()


CHUNKS = 8


def closing_kernel(total_in, scale_in, gain_ref, out_ref, total, scale, result, sems):
    rows = total.shape[0] // CHUNKS

    def copies(i):
        at = pl.ds(i * rows, rows)
        return (
            pltpu.make_async_copy(total_in.at[at, :], total.at[at, :], sems.at[0, i]),
            pltpu.make_async_copy(scale_in.at[at, :], scale.at[at, :], sems.at[1, i]),
            pltpu.make_async_copy(result.at[at, :], out_ref.at[at, :], sems.at[2, i]),
        )

    for i in range(CHUNKS):
        first, second, _ = copies(i)
        first.start()
        second.start()
    for i in range(CHUNKS):
        first, second, third = copies(i)
        first.wait()
        second.wait()
        at = pl.ds(i * rows, rows)
        result[at, :] = (total[at, :].astype(F32) * scale[at, :1] * gain_ref[...]).astype(BF16)
        third.start()
    for i in range(CHUNKS):
        copies(i)[2].wait()


def fused(n, stream_in, decay_shift, mixer_gain, gate_weight, input_weight, filter_taps, recur_gate,
          inlet_gate, decay_param, mixer_out, feedforward_gain, up_weight, down_weight, final_gain):
    _, length, half = stream_in.shape
    shard, channels = gate_weight.shape
    hidden = up_weight.shape[1]
    width = down_weight.shape[1]
    model = shard * n
    blocks = length // ROWS
    half_n = n // 2
    vmem = pl.BlockSpec(memory_space=pltpu.VMEM)
    hbm = pl.BlockSpec(memory_space=pl.ANY)
    swaps = 1 + 2 * blocks + half_n * blocks + blocks
    total, scale = pl.pallas_call(
        functools.partial(layer_kernel, n),
        out_shape=(jax.ShapeDtypeStruct((length, half), BF16), jax.ShapeDtypeStruct((length, 128), F32)),
        in_specs=[hbm, vmem, vmem, hbm, hbm, vmem, vmem, vmem, vmem, hbm, vmem, hbm, hbm],
        out_specs=(hbm, vmem),
        scratch_shapes=[
            pltpu.VMEM((length, half), BF16),
            pltpu.VMEM((model, channels), BF16),
            pltpu.VMEM((model, channels), BF16),
            pltpu.VMEM((n, channels, width), BF16),
            pltpu.VMEM((model, hidden), BF16),
            pltpu.VMEM((n, hidden, width), BF16),
            pltpu.VMEM((length, half), BF16),
            pltpu.VMEM((length, model), BF16),
            pltpu.VMEM((8 + ROWS, channels), F32),
            pltpu.VMEM((8, channels), F32),
            pltpu.VMEM((ROWS, channels), F32),
            pltpu.VMEM((ROWS, channels), F32),
            pltpu.VMEM((2, length, half), BF16),
            pltpu.VMEM((length, half), BF16),
            pltpu.VMEM((length, half), BF16),
            pltpu.VMEM((length, half), BF16),
            pltpu.VMEM((length, hidden), BF16),
            pltpu.VMEM((length, 128), F32),
            pltpu.VMEM((length, 128), F32),
            pltpu.SemaphoreType.DMA((6,)),
            pltpu.SemaphoreType.DMA((9, 3, n - 1)),
            pltpu.SemaphoreType.DMA((9, 3, n - 1)),
            pltpu.SemaphoreType.DMA((swaps,)),
            pltpu.SemaphoreType.DMA((swaps,)),
            pltpu.SemaphoreType.DMA((half_n * blocks,)),
        ],
        compiler_params=pltpu.CompilerParams(
            collective_id=0, has_side_effects=True, vmem_limit_bytes=67043328
        ),
        name="gated_layer",
    )(
        stream_in.reshape(length, half),
        decay_shift,
        mixer_gain.reshape(1, -1),
        gate_weight,
        input_weight,
        filter_taps,
        recur_gate,
        inlet_gate,
        decay_param.reshape(1, -1),
        mixer_out,
        feedforward_gain.reshape(1, -1),
        up_weight,
        down_weight,
    )
    out = pl.pallas_call(
        closing_kernel,
        out_shape=jax.ShapeDtypeStruct((length, half), BF16),
        in_specs=[hbm, hbm, vmem],
        out_specs=hbm,
        scratch_shapes=[
            pltpu.VMEM((length, half), BF16),
            pltpu.VMEM((length, 128), F32),
            pltpu.VMEM((length, half), BF16),
            pltpu.SemaphoreType.DMA((3, CHUNKS)),
        ],
        name="closing",
    )(total, scale, final_gain.reshape(1, -1))
    return out.reshape(1, length, half)


def fits(mesh, n, args):
    num_seq, length, half = args[0].shape
    width = args[9].shape[1]
    shard = args[3].shape[0]
    return (
        mesh.shape["rep"] == 2 and mesh.shape["tp"] == 2 and n % 8 == 0 and num_seq == 1
        and width % 128 == 0 and args[11].shape[1] % 1024 == 0 and length == 4 * ROWS and shard >= 3 * TILE and length % ROWS == 0
    )


def local_for(mesh):
    n = mesh.shape["fs"]

    def local(*args):
        if fits(mesh, n, args):
            return fused(n, *args)
        return plain(*args)

    return local


def solution(mesh):
    return jax.shard_map(
        local_for(mesh),
        mesh=mesh,
        in_specs=(
            P(("rep", "fs"), None, "tp"),
            P(("rep", "fs"), None),
            P(),
            P("fs", "tp"),
            P("fs", "tp"),
            P(None, "tp"),
            P("tp", None, None),
            P("tp", None, None),
            P("tp"),
            P("tp", "fs"),
            P(),
            P("fs", "tp"),
            P("tp", "fs"),
            P("tp"),
        ),
        out_specs=P(("rep", "fs"), None, "tp"),
        check_vma=False,
    )
```

```python
import functools

import jax
import jax.numpy as jnp
from jax import lax
from jax.experimental import pallas as pl
from jax.experimental.pallas import tpu as pltpu
from jax.sharding import PartitionSpec as P

D = 2048


epsilon = 1e-06
rate_scale = 8.0


def norm_rows(values, row_gain):
    mean_sq = jnp.mean(values * values, axis=-1, keepdims=True)
    return values * lax.rsqrt(mean_sq + epsilon) * row_gain


def combine(earlier, later):
    return (earlier[0] * later[0], later[0] * earlier[1] + later[1])


def plain(
    stream_in,
    decay_shift,
    mixer_gain,
    gate_weight,
    input_weight,
    filter_taps,
    recur_gate,
    inlet_gate,
    decay_param,
    mixer_out,
    feedforward_gain,
    up_weight,
    down_weight,
    final_gain,
):
    num_seq, length, half_width = stream_in.shape
    whole = lax.all_gather(stream_in, "tp", axis=2, tiled=True)
    flat_rows = num_seq * length
    normed = norm_rows(whole.reshape(flat_rows, -1).astype(jnp.float32), mixer_gain).astype(
        jnp.bfloat16
    )
    channels = gate_weight.shape[1]
    columns = normed
    gate_logits = jnp.dot(
        columns,
        lax.all_gather(gate_weight, "fs", axis=0, tiled=True),
        preferred_element_type=jnp.float32,
    )
    input_pre = jnp.dot(
        columns,
        lax.all_gather(input_weight, "fs", axis=0, tiled=True),
        preferred_element_type=jnp.float32,
    )
    gate_logits = gate_logits.astype(jnp.bfloat16)
    input_pre = input_pre.astype(jnp.bfloat16)
    branch = jax.nn.gelu(gate_logits.astype(jnp.float32), approximate=True)
    num_taps = filter_taps.shape[0]
    extended_front = jnp.pad(
        input_pre.astype(jnp.float32).reshape(num_seq, length, channels),
        ((0, 0), (num_taps - 1, 0), (0, 0)),
    )
    filtered = jnp.zeros((num_seq, length, channels), jnp.float32)
    for offset in range(num_taps):
        filtered = (
            filtered
            + extended_front[:, offset : offset + length] * filter_taps[offset][None, None, :]
        )
    filtered = filtered.astype(jnp.bfloat16).reshape(flat_rows, channels)
    num_blocks = recur_gate.shape[0]
    grouped = filtered.reshape(flat_rows, num_blocks, recur_gate.shape[1])
    recur = jax.nn.sigmoid(
        jnp.einsum("lni,nij->lnj", grouped, recur_gate, preferred_element_type=jnp.float32).reshape(
            flat_rows, channels
        )
    )
    inlet = jax.nn.sigmoid(
        jnp.einsum("lni,nij->lnj", grouped, inlet_gate, preferred_element_type=jnp.float32).reshape(
            flat_rows, channels
        )
    )
    logarithm_decay = (
        -rate_scale * recur * jax.nn.softplus(-decay_param)[None, :]
        + decay_shift.reshape(flat_rows)[:, None]
    )
    decay = jnp.exp(logarithm_decay).reshape(num_seq, length, channels)
    drive = (
        jnp.sqrt(-jnp.expm1(2.0 * logarithm_decay)) * inlet * filtered.astype(jnp.float32)
    ).reshape(num_seq, length, channels)
    states = lax.associative_scan(combine, (decay, drive), axis=1)[1]
    mixed = (states.reshape(flat_rows, channels) * branch).astype(jnp.bfloat16)
    mixer_terms = (
        jnp.dot(
            mixed,
            lax.all_gather(mixer_out, "fs", axis=1, tiled=True),
            preferred_element_type=jnp.float32,
        )
        .astype(jnp.bfloat16)
        .astype(jnp.float32)
    )
    mixer_sum = lax.psum_scatter(
        mixer_terms.astype(jnp.bfloat16), "tp", scatter_dimension=1, tiled=True
    ).astype(jnp.float32)
    stream_mid = (stream_in.reshape(flat_rows, half_width).astype(jnp.float32) + mixer_sum).astype(
        jnp.bfloat16
    )
    stream_whole = lax.all_gather(stream_mid, "tp", axis=1, tiled=True)
    normed_mid = norm_rows(stream_whole.astype(jnp.float32), feedforward_gain).astype(jnp.bfloat16)
    columns = normed_mid
    up_proj = jnp.dot(
        columns,
        lax.all_gather(up_weight, "fs", axis=0, tiled=True),
        preferred_element_type=jnp.float32,
    )
    activated = jnp.square(jax.nn.relu(up_proj)).astype(jnp.bfloat16)
    ffn_terms = (
        jnp.dot(
            activated,
            lax.all_gather(down_weight, "fs", axis=1, tiled=True),
            preferred_element_type=jnp.float32,
        )
        .astype(jnp.bfloat16)
        .astype(jnp.float32)
    )
    ffn_sum = lax.psum_scatter(
        ffn_terms.astype(jnp.bfloat16), "tp", scatter_dimension=1, tiled=True
    ).astype(jnp.float32)
    total = stream_mid.astype(jnp.float32) + ffn_sum
    squares_sum = lax.psum(jnp.sum(total * total, axis=1), "tp")
    layer_out = total * lax.rsqrt(squares_sum / D + epsilon)[:, None] * final_gain[None, :]
    return layer_out.astype(jnp.bfloat16).reshape(num_seq, length, half_width)


F32 = jnp.float32
BF16 = jnp.bfloat16
TILE = 16
FORE, BACK, BOTH = range(3)
ROWS = 256


def split_rows(rows, up):
    third = rows // 3 // TILE * TILE + (TILE if up else 0)
    return rows - 2 * third, third


def expm1_neg(v):
    series = -v * (1.0 + v * (1 / 2) * (1.0 + v * (1 / 3) * (1.0 + v * (1 / 4) * (1.0 + v * (1 / 5) * (1.0 + v * (1 / 6))))))
    return jnp.where(v > -0.25, series, 1.0 - jnp.exp(v))


def layer_kernel(
    n,
    x_in, shift_in, mgain_in, wg_in, wi_in, taps_in, rg_in, ig_in, sp_in, wo_in,
    fgain_in, wu_in, wd_in, lgain_in,
    out_ref, scale_ref,
    shift_ref, mgain_ref, taps_ref, rg_ref, ig_ref, sp_ref, fgain_ref, lgain_ref,
    x_ref, wg, wi, wo, wu, wd, other, normed, front, carry, scan_a, scan_b, part, prec, mid, mid_other,
    act, sq_send, sq_recv, acc, scales,
    local_sems, send_sems, recv_sems, tp_send, tp_recv, out_sems,
):
    rep, fs, tp = lax.axis_index("rep"), lax.axis_index("fs"), lax.axis_index("tp")
    half_n = n // 2
    length, half = x_in.shape
    channels = wg.shape[1]
    width = wd.shape[2]
    shard = wg_in.shape[0]
    hidden = wu.shape[1]
    blocks = length // ROWS

    def ring_to_fs(p):
        p = lax.rem(p + 2 * n, n)
        return jnp.where(p < half_n, 2 * p, 2 * (n - 1 - p) + 1)

    odd = lax.rem(fs, 2)
    pos = (1 - odd) * (fs // 2) + odd * (n - 1 - fs // 2)
    right, left = ring_to_fs(pos + 1), ring_to_fs(pos - 1)

    def by_row(dst, lo, cols):
        def view(owner, off, size):
            return dst.at[pl.ds(pl.multiple_of(owner * shard + off, TILE), size), pl.ds(lo, cols)]
        return view

    def by_owner(dst, lo):
        def view(owner, off, size):
            return dst.at[owner, pl.ds(pl.multiple_of(lo + off, TILE), size), :]
        return view

    rows_o, rows_d = wo.shape[1], wd.shape[1]
    def plain_split(rows, up):
        p, q = split_rows(rows, up)
        return (0, p), (p, q)

    quarter = hidden // 4
    half_d = rows_d // 2
    private, last = rows_d // 8, rows_d // 16
    common = half_d - 2 * private - last
    views = [
        (by_row(wg, 0, channels), BACK, plain_split(shard, True)),
        (by_row(wi, 0, channels), FORE, plain_split(shard, True)),
        (by_owner(wo, 0), FORE, plain_split(rows_o, True)),
        (by_row(wu, 0, quarter), BACK, plain_split(shard, True)),
        (by_row(wu, quarter, 2 * quarter), FORE, plain_split(shard, True)),
        (by_row(wu, 3 * quarter, quarter), BACK, plain_split(shard, True)),
        (by_owner(wd, 0), FORE, ((0, common), (half_d, private))),
        (by_owner(wd, 0), BACK, ((half_d + 2 * private, common), (common + last, private))),
        (by_owner(wd, 0), BOTH, ((common, last), (rows_d - last, last))),
    ]
    ups = range(3, 6)
    downs = range(6, 9)

    def remote(view, k, lane, s, device):
        return pltpu.make_async_remote_copy(
            src_ref=view, dst_ref=view, send_sem=send_sems.at[k, lane, s],
            recv_sem=recv_sems.at[k, lane, s], device_id=device,
            device_id_type=pl.DeviceIdType.MESH,
        )

    def cw(k, s, shift=0):
        view, role, (whole, (lo, size)) = views[k]
        at = (lo + rep * size, size) if role == BACK else whole
        return remote(view(ring_to_fs(pos - s - shift), *at), k, 0, s, {"fs": right})

    def ccw(k, s, shift=0):
        view, role, (whole, (lo, size)) = views[k]
        at = whole if role == BACK else (lo + rep * size if role == FORE else lo, size)
        return remote(view(ring_to_fs(pos + s + shift), *at), k, 1, s, {"fs": left})

    def across(k, s, side):
        view, role, (_, (lo, size)) = views[k]
        owner = pos + s + 1 if role == FORE else pos - s - 1
        return remote(view(ring_to_fs(owner), lo + side * size, size), k, 2, s, {"rep": 1 - rep})

    def shared(k):
        return views[k][1] != BOTH

    def begin(k):
        cw(k, 0).start()
        ccw(k, 0).start()

    def service(k, s, last):
        def forward(make):
            if last is None:
                pl.when(s + 1 < n - 1)(lambda: make(k, s + 1).start())
            elif not last:
                make(k, s + 1).start()

        cw(k, s, 1).wait_recv()
        forward(cw)
        if views[k][1] == BACK:
            across(k, s, rep).start()
        ccw(k, s, 1).wait_recv()
        forward(ccw)
        if views[k][1] == FORE:
            across(k, s, rep).start()

    def wait_across(k, s):
        if shared(k):
            across(k, s, 1 - rep).wait_recv()

    def swap(src, dst, index):
        return pltpu.make_async_remote_copy(
            src_ref=src, dst_ref=dst, send_sem=tp_send.at[index], recv_sem=tp_recv.at[index],
            device_id={"tp": 1 - tp}, device_id_type=pl.DeviceIdType.MESH,
        )

    own = [
        (x_in, x_ref),
        (wg_in, wg.at[pl.ds(pl.multiple_of(fs * shard, TILE), shard), :]),
        (wi_in, wi.at[pl.ds(pl.multiple_of(fs * shard, TILE), shard), :]),
        (wo_in, wo.at[fs]),
        (wu_in, wu.at[pl.ds(pl.multiple_of(fs * shard, TILE), shard), :]),
        (wd_in, wd.at[fs]),
        (mgain_in, mgain_ref),
        (shift_in, shift_ref),
        (taps_in, taps_ref),
        (rg_in, rg_ref),
        (ig_in, ig_ref),
        (sp_in, sp_ref),
        (fgain_in, fgain_ref),
        (lgain_in, lgain_ref),
    ]
    local = [pltpu.make_async_copy(a, b, local_sems.at[i]) for i, (a, b) in enumerate(own)]
    barrier = pltpu.get_barrier_semaphore()
    for device in ({"fs": right}, {"fs": left}, {"rep": 1 - rep}, {"tp": 1 - tp}):
        pl.semaphore_signal(barrier, inc=1, device_id=device, device_id_type=pl.DeviceIdType.MESH)
    for i in (1, 2, 3, 0, 4, 5, *range(6, len(own))):
        local[i].start()
    pl.semaphore_wait(barrier, 4)
    swap_x = swap(x_ref, other, 0)
    for k in range(3):
        local[1 + k].wait()
        begin(k)
    local[0].wait()
    swap_x.start()
    for i in range(4, len(own)):
        local[i].wait()

    own_cols = pl.ds(pl.multiple_of(tp * half, 128), half)
    other_cols = pl.ds(pl.multiple_of((1 - tp) * half, 128), half)

    def norm_block(first, second, gain_ref, rows):
        a = first[rows, :].astype(F32)
        b = second[rows, :].astype(F32)
        mean = (jnp.sum(a * a, axis=1, keepdims=True) + jnp.sum(b * b, axis=1, keepdims=True)) / (2 * half)
        scale = lax.rsqrt(mean + epsilon)
        normed[rows, own_cols] = (a * scale * gain_ref[:, own_cols]).astype(BF16)
        normed[rows, other_cols] = (b * scale * gain_ref[:, other_cols]).astype(BF16)

    small = 64

    pieces = length // small
    share = -(-pieces // (n - 2))

    @pl.loop(0, n - 2)
    def _(s):
        for k in range(3):
            service(k, s, False)
        pl.when(s == 0)(swap_x.wait)
        for k in list(ups)[:2]:
            pl.when(s == n - 3)(functools.partial(begin, k))
        for piece in range(share):
            i = s * share + piece

            @pl.when(i < pieces)
            def _():
                norm_block(x_ref, other, mgain_ref, pl.ds(pl.multiple_of(i * small, small), small))

    begin(ups[-1])
    for k in range(3):
        service(k, n - 2, True)

    lead = n - 2

    def tick(t, j):
        pl.when(t < n - 1)(lambda: service(ups[j], t, None))
        if j == 2:
            for e, k in enumerate(downs):
                pl.when(t == (n - 4 if e == 0 else n - 3))(functools.partial(begin, k))
        pl.when(t >= lead)(lambda: service(downs[j], t - lead, None))

    for j in range(3):
        tick(0, j)

    @pl.loop(0, n - 1)
    def _(s):
        for k in range(3):
            wait_across(k, s)

    front[pl.ds(0, 8), :] = jnp.zeros((8, channels), F32)
    carry[...] = jnp.zeros_like(carry)
    decay_param = sp_ref[...]
    rate = rate_scale * (jnp.maximum(-decay_param, 0.0) + jnp.log1p(jnp.exp(-jnp.abs(decay_param))))
    num_taps = taps_ref.shape[0]
    groups = rg_ref.shape[0]
    block = rg_ref.shape[1]
    @pl.loop(0, blocks)
    def _(i):
        rows = pl.ds(pl.multiple_of(i * ROWS, ROWS), ROWS)
        tick(i + 1, 0)
        cols = normed[rows, :]
        front[pl.ds(8, ROWS), :] = jnp.dot(cols, wi[...], preferred_element_type=F32).astype(BF16).astype(F32)
        gate = jnp.dot(cols, wg[...], preferred_element_type=F32).astype(BF16)
        shift = jnp.transpose(jnp.broadcast_to(shift_ref[:, rows], (128, ROWS)))[:, :1]
        for g in range(groups):
            if g == 1:
                tick(i + 1, 1)
            ch = slice(g * block, (g + 1) * block)
            window = front[:, ch]
            filtered = jnp.zeros((ROWS, block), F32)
            for tap in range(num_taps):
                back = num_taps - 1 - tap
                moved = window if back == 0 else pltpu.roll(window, back, 0)
                filtered = filtered + moved[8:] * taps_ref[tap : tap + 1, ch]
            filtered = filtered.astype(BF16)
            recur = jax.nn.sigmoid(jnp.dot(filtered, rg_ref[g], preferred_element_type=F32))
            inlet = jax.nn.sigmoid(jnp.dot(filtered, ig_ref[g], preferred_element_type=F32))
            log_decay = shift - recur * rate[:, ch]
            a = jnp.exp(log_decay)
            b = jnp.sqrt(expm1_neg(2.0 * log_decay)) * inlet * filtered.astype(F32)
            a = a.reshape(ROWS // 8, 8, block)
            b = b.reshape(ROWS // 8, 8, block)
            at = lax.broadcasted_iota(jnp.int32, (ROWS // 8, 8, block), 1)
            for back in (1, 2, 4):
                keep = at >= back
                b = jnp.where(keep, a * pltpu.roll(b, back, 1) + b, b)
                a = jnp.where(keep, a * pltpu.roll(a, back, 1), a)
            scan_a[:, ch] = a.reshape(ROWS, block)
            scan_b[:, ch] = b.reshape(ROWS, block)
        front[pl.ds(0, 8), :] = front[pl.ds(ROWS, 8), :]

        def step_scan(t, h):
            at = pl.ds(pl.multiple_of(t * 8, 8), 8)
            states = scan_a[at, :] * h + scan_b[at, :]
            scan_b[at, :] = states
            return jnp.broadcast_to(states[7:8, :], states.shape)

        carry[...] = lax.fori_loop(0, ROWS // 8, step_scan, carry[...], unroll=4)
        tick(i + 1, 2)
        mixed = (scan_b[...] * jax.nn.gelu(gate.astype(F32), approximate=True)).astype(BF16)
        for j in range(half_n):
            to = pl.ds(j * width, width)
            part[1, rows, to] = jnp.dot(mixed, wo[(1 - tp) * half_n + j], preferred_element_type=F32).astype(BF16)
        swap(part.at[1, rows, :], prec.at[rows, :], 1 + i).start()
        for j in range(half_n):
            to = pl.ds(j * width, width)
            part[0, rows, to] = jnp.dot(mixed, wo[tp * half_n + j], preferred_element_type=F32).astype(BF16)

    tick(blocks + 1, 0)

    @pl.loop(0, blocks)
    def _(i):
        rows = pl.ds(pl.multiple_of(i * ROWS, ROWS), ROWS)
        swap(part.at[1, rows, :], prec.at[rows, :], 1 + i).wait()
        mid[rows, :] = (
            x_ref[rows, :].astype(F32) + (part[0, rows, :].astype(F32) + prec[rows, :].astype(F32))
        ).astype(BF16)
        swap(mid.at[rows, :], mid_other.at[rows, :], 1 + blocks + i).start()

    tick(blocks + 1, 1)

    @pl.loop(0, blocks)
    def _(i):
        rows = pl.ds(pl.multiple_of(i * ROWS, ROWS), ROWS)
        swap(mid.at[rows, :], mid_other.at[rows, :], 1 + blocks + i).wait()

    tick(blocks + 1, 2)

    for part_of in range(2):

        @pl.loop(part_of * (pieces // 2), (part_of + 1) * (pieces // 2))
        def _(i):
            norm_block(mid, mid_other, fgain_ref, pl.ds(pl.multiple_of(i * small, small), small))

        tick(blocks + 2, part_of)

    tick(blocks + 2, 2)
    for t in range(blocks + 3, n + 1):
        for j in range(3):
            tick(t, j)

    @pl.loop(0, n - 1)
    def _(s):
        for k in ups:
            wait_across(k, s)

    up_cols = min(512, hidden)
    @pl.loop(0, hidden // up_cols)
    def _(c):
        to = pl.ds(pl.multiple_of(c * up_cols, up_cols), up_cols)

        @pl.loop(0, blocks)
        def _(i):
            rows = pl.ds(pl.multiple_of(i * ROWS, ROWS), ROWS)
            up = jnp.maximum(jnp.dot(normed[rows, :], wu[:, to], preferred_element_type=F32), 0.0)
            act[rows, to] = (up * up).astype(BF16)

        for j in range(3):
            pl.when(c == j)(functools.partial(tick, n + 1, j))

    tick(n + 2, 0)

    def place(owner, i):
        column = lax.rem(owner, half_n)
        slot = lax.rem(owner // half_n + tp, 2)
        rows = pl.ds(pl.multiple_of(i * ROWS, ROWS), ROWS)
        to = pl.ds(pl.multiple_of(column * width, 128), width)
        return column, slot, rows, to

    def back_swap(column, i):
        _, _, rows, to = place(column, i)
        return swap(part.at[1, rows, to], prec.at[rows, to], 1 + 2 * blocks + column * blocks + i)

    def write(column, i):
        _, _, rows, to = place(column, i)
        return pltpu.make_async_copy(other.at[rows, to], out_ref.at[rows, to], out_sems.at[column * blocks + i])

    def down_rows(owner, i):
        column, slot, rows, to = place(owner, i)
        part[slot, rows, to] = jnp.dot(act[rows, :], wd[owner], preferred_element_type=F32).astype(BF16)
        pl.when(slot == 1)(lambda: back_swap(column, i).start())

    def early_rows(e, owner, i):
        rows = pl.ds(pl.multiple_of(i * ROWS, ROWS), ROWS)
        take = pl.ds((1 - e) * half_d, half_d)
        acc[e, rows, :] = jnp.dot(act[rows, take], wd[owner, take, :], preferred_element_type=F32)

    def late_rows(e, owner, i):
        column, slot, rows, to = place(owner, i)
        take = pl.ds(e * half_d, half_d)
        rest = jnp.dot(act[rows, take], wd[owner, take, :], preferred_element_type=F32)
        part[slot, rows, to] = (acc[e, rows, :] + rest).astype(BF16)
        pl.when(slot == 1)(lambda: back_swap(column, i).start())

    def total_rows(owner, i):
        column, slot, rows, to = place(owner, i)

        @pl.when(slot == 0)
        def _():
            back_swap(column, i).wait_recv()
            total = mid[rows, to].astype(F32) + (part[0, rows, to].astype(F32) + prec[rows, to].astype(F32))
            other[rows, to] = (total * lgain_ref[:, to]).astype(BF16)
            squares = total * total
            sq_send[rows, :] += sum(squares[:, at : at + 128] for at in range(0, width, 128))
            write(column, i).start()

    def over_rows(*makes):
        @pl.loop(0, blocks)
        def _(i):
            for make, owner in makes:
                make(owner, i)

    order = [ring_to_fs(pos + ahead) for ahead in [0, half_n]]
    for s in range(half_n, n - 1):
        order += [ring_to_fs(pos - s - 1), ring_to_fs(pos + s + 1)]
    sq_send[...] = jnp.zeros_like(sq_send)
    over_rows((down_rows, order[0]))
    for at in range(3 * n + 7, 3 * (lead + half_n + 1)):
        tick(at // 3, at % 3)
    for s in range(half_n - 1, n - 1):
        ahead = lead + s + 2
        for earlier in range(half_n) if s == half_n - 1 else [s]:
            for k in downs:
                wait_across(k, earlier)
        if s == half_n - 1:
            over_rows((down_rows, order[1]), (total_rows, order[0]))
        elif s < n - 2:
            at = 2 * (s - half_n + 1)
            over_rows((down_rows, order[at]), (total_rows, order[at - 1]))
            if s < n - 3:
                tick(ahead, 0)
            over_rows((down_rows, order[at + 1]), (total_rows, order[at]))
        if s < n - 3:
            for j in range(1 if s >= half_n else 0, 3):
                tick(ahead, j)
                if s == half_n - 1 and j < 2:
                    over_rows((functools.partial(early_rows, j), order[j - 2]))

    def swap_sq(i):
        rows = pl.ds(pl.multiple_of(i * ROWS, ROWS), ROWS)
        return swap(sq_send.at[rows, :], sq_recv.at[rows, :], 1 + 2 * blocks + half_n * blocks + i)

    def settle(i):
        total_rows(order[-2], i)
        total_rows(order[-1], i)
        swap_sq(i).start()

    @pl.loop(0, blocks)
    def _(i):
        late_rows(0, order[-2], i)
        late_rows(1, order[-1], i)
        total_rows(order[-3], i)
        pl.when(i > 0)(lambda: settle(i - 1))

    settle(blocks - 1)

    def write_scale(i):
        rows = pl.ds(pl.multiple_of(i * ROWS, ROWS), ROWS)
        return pltpu.make_async_copy(scales.at[rows, :], scale_ref.at[rows, :], out_sems.at[half_n * blocks + i])

    @pl.loop(0, blocks)
    def _(i):
        swap_sq(i).wait()
        rows = pl.ds(pl.multiple_of(i * ROWS, ROWS), ROWS)
        squares = jnp.sum(sq_send[rows, :] + sq_recv[rows, :], axis=1, keepdims=True)
        scales[rows, :] = jnp.broadcast_to(lax.rsqrt(squares / (2 * half) + epsilon), (ROWS, 128))
        write_scale(i).start()

    @pl.loop(0, n - 1)
    def _(s):
        for k in range(len(views)):
            cw(k, s).wait_send()
            ccw(k, s).wait_send()
            if shared(k):
                across(k, s, rep).wait_send()

    @pl.loop(0, blocks)
    def _(i):
        for j in range(half_n):
            back_swap(j, i).wait_send()
            write(j, i).wait()
        write_scale(i).wait()


CHUNKS = 8


def closing_kernel(total_in, scale_in, out_ref, total, scale, result, sems):
    rows = total.shape[0] // CHUNKS

    def copies(i):
        at = pl.ds(i * rows, rows)
        return (
            pltpu.make_async_copy(total_in.at[at, :], total.at[at, :], sems.at[0, i]),
            pltpu.make_async_copy(scale_in.at[at, :], scale.at[at, :], sems.at[1, i]),
            pltpu.make_async_copy(result.at[at, :], out_ref.at[at, :], sems.at[2, i]),
        )

    for i in range(CHUNKS):
        first, second, _ = copies(i)
        first.start()
        second.start()
    for i in range(CHUNKS):
        first, second, third = copies(i)
        first.wait()
        second.wait()
        at = pl.ds(i * rows, rows)
        result[at, :] = (total[at, :].astype(F32) * scale[at, :1]).astype(BF16)
        third.start()
    for i in range(CHUNKS):
        copies(i)[2].wait()


def fused(n, stream_in, decay_shift, mixer_gain, gate_weight, input_weight, filter_taps, recur_gate,
          inlet_gate, decay_param, mixer_out, feedforward_gain, up_weight, down_weight, final_gain):
    _, length, half = stream_in.shape
    shard, channels = gate_weight.shape
    hidden = up_weight.shape[1]
    width = down_weight.shape[1]
    model = shard * n
    blocks = length // ROWS
    half_n = n // 2
    vmem = pl.BlockSpec(memory_space=pltpu.VMEM)
    hbm = pl.BlockSpec(memory_space=pl.ANY)
    swaps = 1 + 2 * blocks + half_n * blocks + blocks
    total, scale = pl.pallas_call(
        functools.partial(layer_kernel, n),
        out_shape=(jax.ShapeDtypeStruct((length, half), BF16), jax.ShapeDtypeStruct((length, 128), F32)),
        in_specs=[hbm] * 14,
        out_specs=(hbm, hbm),
        scratch_shapes=[
            pltpu.VMEM((1, length), F32),
            pltpu.VMEM((1, model), F32),
            pltpu.VMEM(filter_taps.shape, F32),
            pltpu.VMEM(recur_gate.shape, BF16),
            pltpu.VMEM(inlet_gate.shape, BF16),
            pltpu.VMEM((1, channels), F32),
            pltpu.VMEM((1, model), F32),
            pltpu.VMEM((1, half), F32),
            pltpu.VMEM((length, half), BF16),
            pltpu.VMEM((model, channels), BF16),
            pltpu.VMEM((model, channels), BF16),
            pltpu.VMEM((n, channels, width), BF16),
            pltpu.VMEM((model, hidden), BF16),
            pltpu.VMEM((n, hidden, width), BF16),
            pltpu.VMEM((length, half), BF16),
            pltpu.VMEM((length, model), BF16),
            pltpu.VMEM((8 + ROWS, channels), F32),
            pltpu.VMEM((8, channels), F32),
            pltpu.VMEM((ROWS, channels), F32),
            pltpu.VMEM((ROWS, channels), F32),
            pltpu.VMEM((2, length, half), BF16),
            pltpu.VMEM((length, half), BF16),
            pltpu.VMEM((length, half), BF16),
            pltpu.VMEM((length, half), BF16),
            pltpu.VMEM((length, hidden), BF16),
            pltpu.VMEM((length, 128), F32),
            pltpu.VMEM((length, 128), F32),
            pltpu.VMEM((2, length, width), F32),
            pltpu.VMEM((length, 128), F32),
            pltpu.SemaphoreType.DMA((14,)),
            pltpu.SemaphoreType.DMA((9, 3, n - 1)),
            pltpu.SemaphoreType.DMA((9, 3, n - 1)),
            pltpu.SemaphoreType.DMA((swaps,)),
            pltpu.SemaphoreType.DMA((swaps,)),
            pltpu.SemaphoreType.DMA((half_n * blocks + blocks,)),
        ],
        compiler_params=pltpu.CompilerParams(
            collective_id=0, has_side_effects=True, vmem_limit_bytes=67043328
        ),
        name="gated_layer",
    )(
        stream_in.reshape(length, half),
        decay_shift,
        mixer_gain.reshape(1, -1),
        gate_weight,
        input_weight,
        filter_taps,
        recur_gate,
        inlet_gate,
        decay_param.reshape(1, -1),
        mixer_out,
        feedforward_gain.reshape(1, -1),
        up_weight,
        down_weight,
        final_gain.reshape(1, -1),
    )
    out = pl.pallas_call(
        closing_kernel,
        out_shape=jax.ShapeDtypeStruct((length, half), BF16),
        in_specs=[hbm, hbm],
        out_specs=hbm,
        scratch_shapes=[
            pltpu.VMEM((length, half), BF16),
            pltpu.VMEM((length, 128), F32),
            pltpu.VMEM((length, half), BF16),
            pltpu.SemaphoreType.DMA((3, CHUNKS)),
        ],
        name="closing",
    )(total, scale)
    return out.reshape(1, length, half)


def fits(mesh, n, args):
    num_seq, length, half = args[0].shape
    width = args[9].shape[1]
    shard = args[3].shape[0]
    return (
        mesh.shape["rep"] == 2 and mesh.shape["tp"] == 2 and n % 8 == 0 and num_seq == 1
        and width % 128 == 0 and args[11].shape[1] % 1024 == 0 and length == 4 * ROWS and shard >= 3 * TILE and length % ROWS == 0
    )


def local_for(mesh):
    n = mesh.shape["fs"]

    def local(*args):
        if fits(mesh, n, args):
            return fused(n, *args)
        return plain(*args)

    return local


def solution(mesh):
    return jax.shard_map(
        local_for(mesh),
        mesh=mesh,
        in_specs=(
            P(("rep", "fs"), None, "tp"),
            P(("rep", "fs"), None),
            P(),
            P("fs", "tp"),
            P("fs", "tp"),
            P(None, "tp"),
            P("tp", None, None),
            P("tp", None, None),
            P("tp"),
            P("tp", "fs"),
            P(),
            P("fs", "tp"),
            P("tp", "fs"),
            P("tp"),
        ),
        out_specs=P(("rep", "fs"), None, "tp"),
        check_vma=False,
    )
```

```python
import functools

import jax
import jax.numpy as jnp
from jax import lax
from jax.experimental import pallas as pl
from jax.experimental.pallas import tpu as pltpu
from jax.sharding import PartitionSpec as P

D = 2048


epsilon = 1e-06
rate_scale = 8.0


def norm_rows(values, row_gain):
    mean_sq = jnp.mean(values * values, axis=-1, keepdims=True)
    return values * lax.rsqrt(mean_sq + epsilon) * row_gain


def combine(earlier, later):
    return (earlier[0] * later[0], later[0] * earlier[1] + later[1])


def plain(
    stream_in,
    decay_shift,
    mixer_gain,
    gate_weight,
    input_weight,
    filter_taps,
    recur_gate,
    inlet_gate,
    decay_param,
    mixer_out,
    feedforward_gain,
    up_weight,
    down_weight,
    final_gain,
):
    num_seq, length, half_width = stream_in.shape
    whole = lax.all_gather(stream_in, "tp", axis=2, tiled=True)
    flat_rows = num_seq * length
    normed = norm_rows(whole.reshape(flat_rows, -1).astype(jnp.float32), mixer_gain).astype(
        jnp.bfloat16
    )
    channels = gate_weight.shape[1]
    columns = normed
    gate_logits = jnp.dot(
        columns,
        lax.all_gather(gate_weight, "fs", axis=0, tiled=True),
        preferred_element_type=jnp.float32,
    )
    input_pre = jnp.dot(
        columns,
        lax.all_gather(input_weight, "fs", axis=0, tiled=True),
        preferred_element_type=jnp.float32,
    )
    gate_logits = gate_logits.astype(jnp.bfloat16)
    input_pre = input_pre.astype(jnp.bfloat16)
    branch = jax.nn.gelu(gate_logits.astype(jnp.float32), approximate=True)
    num_taps = filter_taps.shape[0]
    extended_front = jnp.pad(
        input_pre.astype(jnp.float32).reshape(num_seq, length, channels),
        ((0, 0), (num_taps - 1, 0), (0, 0)),
    )
    filtered = jnp.zeros((num_seq, length, channels), jnp.float32)
    for offset in range(num_taps):
        filtered = (
            filtered
            + extended_front[:, offset : offset + length] * filter_taps[offset][None, None, :]
        )
    filtered = filtered.astype(jnp.bfloat16).reshape(flat_rows, channels)
    num_blocks = recur_gate.shape[0]
    grouped = filtered.reshape(flat_rows, num_blocks, recur_gate.shape[1])
    recur = jax.nn.sigmoid(
        jnp.einsum("lni,nij->lnj", grouped, recur_gate, preferred_element_type=jnp.float32).reshape(
            flat_rows, channels
        )
    )
    inlet = jax.nn.sigmoid(
        jnp.einsum("lni,nij->lnj", grouped, inlet_gate, preferred_element_type=jnp.float32).reshape(
            flat_rows, channels
        )
    )
    logarithm_decay = (
        -rate_scale * recur * jax.nn.softplus(-decay_param)[None, :]
        + decay_shift.reshape(flat_rows)[:, None]
    )
    decay = jnp.exp(logarithm_decay).reshape(num_seq, length, channels)
    drive = (
        jnp.sqrt(-jnp.expm1(2.0 * logarithm_decay)) * inlet * filtered.astype(jnp.float32)
    ).reshape(num_seq, length, channels)
    states = lax.associative_scan(combine, (decay, drive), axis=1)[1]
    mixed = (states.reshape(flat_rows, channels) * branch).astype(jnp.bfloat16)
    mixer_terms = (
        jnp.dot(
            mixed,
            lax.all_gather(mixer_out, "fs", axis=1, tiled=True),
            preferred_element_type=jnp.float32,
        )
        .astype(jnp.bfloat16)
        .astype(jnp.float32)
    )
    mixer_sum = lax.psum_scatter(
        mixer_terms.astype(jnp.bfloat16), "tp", scatter_dimension=1, tiled=True
    ).astype(jnp.float32)
    stream_mid = (stream_in.reshape(flat_rows, half_width).astype(jnp.float32) + mixer_sum).astype(
        jnp.bfloat16
    )
    stream_whole = lax.all_gather(stream_mid, "tp", axis=1, tiled=True)
    normed_mid = norm_rows(stream_whole.astype(jnp.float32), feedforward_gain).astype(jnp.bfloat16)
    columns = normed_mid
    up_proj = jnp.dot(
        columns,
        lax.all_gather(up_weight, "fs", axis=0, tiled=True),
        preferred_element_type=jnp.float32,
    )
    activated = jnp.square(jax.nn.relu(up_proj)).astype(jnp.bfloat16)
    ffn_terms = (
        jnp.dot(
            activated,
            lax.all_gather(down_weight, "fs", axis=1, tiled=True),
            preferred_element_type=jnp.float32,
        )
        .astype(jnp.bfloat16)
        .astype(jnp.float32)
    )
    ffn_sum = lax.psum_scatter(
        ffn_terms.astype(jnp.bfloat16), "tp", scatter_dimension=1, tiled=True
    ).astype(jnp.float32)
    total = stream_mid.astype(jnp.float32) + ffn_sum
    squares_sum = lax.psum(jnp.sum(total * total, axis=1), "tp")
    layer_out = total * lax.rsqrt(squares_sum / D + epsilon)[:, None] * final_gain[None, :]
    return layer_out.astype(jnp.bfloat16).reshape(num_seq, length, half_width)


F32 = jnp.float32
BF16 = jnp.bfloat16
TILE = 16
FORE, BACK, BOTH = range(3)
ROWS = 256


def split_rows(rows, up):
    third = rows // 3 // TILE * TILE + (TILE if up else 0)
    return rows - 2 * third, third


def expm1_neg(v):
    series = -v * (1.0 + v * (1 / 2) * (1.0 + v * (1 / 3) * (1.0 + v * (1 / 4) * (1.0 + v * (1 / 5) * (1.0 + v * (1 / 6))))))
    return jnp.where(v > -0.25, series, 1.0 - jnp.exp(v))


def layer_kernel(
    n,
    x_in, shift_in, mgain_in, wg_in, wi_in, taps_in, rg_in, ig_in, sp_in, wo_in,
    fgain_in, wu_in, wd_in, lgain_in,
    out_ref, scale_ref,
    shift_ref, mgain_ref, taps_ref, rg_ref, ig_ref, sp_ref, fgain_ref, lgain_ref,
    x_ref, wg, wi, wo, wu, wd, other, normed, front, carry, scan_a, scan_b, part, prec, mid, mid_other,
    act, sq_send, sq_recv, acc, scales,
    local_sems, send_sems, recv_sems, tp_send, tp_recv, out_sems,
):
    rep, fs, tp = lax.axis_index("rep"), lax.axis_index("fs"), lax.axis_index("tp")
    half_n = n // 2
    length, half = x_in.shape
    channels = wg.shape[1]
    width = wd.shape[2]
    shard = wg_in.shape[0]
    hidden = wu.shape[1]
    blocks = length // ROWS

    def ring_to_fs(p):
        p = lax.rem(p + 2 * n, n)
        return jnp.where(p < half_n, 2 * p, 2 * (n - 1 - p) + 1)

    odd = lax.rem(fs, 2)
    pos = (1 - odd) * (fs // 2) + odd * (n - 1 - fs // 2)
    right, left = ring_to_fs(pos + 1), ring_to_fs(pos - 1)

    def by_row(dst, lo, cols):
        def view(owner, off, size):
            return dst.at[pl.ds(pl.multiple_of(owner * shard + off, TILE), size), pl.ds(lo, cols)]
        return view

    def by_owner(dst, lo):
        def view(owner, off, size):
            return dst.at[owner, pl.ds(pl.multiple_of(lo + off, TILE), size), :]
        return view

    rows_o, rows_d = wo.shape[1], wd.shape[1]
    def plain_split(rows, up):
        p, q = split_rows(rows, up)
        return (0, p), (p, q)

    quarter = hidden // 4
    half_d = rows_d // 2
    private, last = rows_d // 8, rows_d // 16
    common = half_d - 2 * private - last
    views = [
        (by_row(wg, 0, channels), BACK, plain_split(shard, True)),
        (by_row(wi, 0, channels), FORE, plain_split(shard, True)),
        (by_owner(wo, 0), FORE, plain_split(rows_o, True)),
        (by_row(wu, 0, quarter), BACK, plain_split(shard, True)),
        (by_row(wu, quarter, 2 * quarter), FORE, plain_split(shard, True)),
        (by_row(wu, 3 * quarter, quarter), BACK, plain_split(shard, True)),
        (by_owner(wd, 0), FORE, ((0, common), (half_d, private))),
        (by_owner(wd, 0), BACK, ((half_d + 2 * private, common), (common + last, private))),
        (by_owner(wd, 0), BOTH, ((common, last), (rows_d - last, last))),
    ]
    ups = range(3, 6)
    downs = range(6, 9)

    def remote(view, k, lane, s, device):
        return pltpu.make_async_remote_copy(
            src_ref=view, dst_ref=view, send_sem=send_sems.at[k, lane, s],
            recv_sem=recv_sems.at[k, lane, s], device_id=device,
            device_id_type=pl.DeviceIdType.MESH,
        )

    def cw(k, s, shift=0):
        view, role, (whole, (lo, size)) = views[k]
        at = (lo + rep * size, size) if role == BACK else whole
        return remote(view(ring_to_fs(pos - s - shift), *at), k, 0, s, {"fs": right})

    def ccw(k, s, shift=0):
        view, role, (whole, (lo, size)) = views[k]
        at = whole if role == BACK else (lo + rep * size if role == FORE else lo, size)
        return remote(view(ring_to_fs(pos + s + shift), *at), k, 1, s, {"fs": left})

    def across(k, s, side):
        view, role, (_, (lo, size)) = views[k]
        owner = pos + s + 1 if role == FORE else pos - s - 1
        return remote(view(ring_to_fs(owner), lo + side * size, size), k, 2, s, {"rep": 1 - rep})

    def shared(k):
        return views[k][1] != BOTH

    def begin(k):
        cw(k, 0).start()
        ccw(k, 0).start()

    def service(turns, s, last):
        for make, k in turns:
            make(k, s, 1).wait_recv()
            if last is None:
                pl.when(s + 1 < n - 1)(functools.partial(lambda make, k: make(k, s + 1).start(), make, k))
            elif not last:
                make(k, s + 1).start()
            if views[k][1] == (BACK if make is cw else FORE):
                across(k, s, rep).start()

    def turns_of(back, fore, third):
        return [[(cw, back), (ccw, fore)], [(cw, fore), (ccw, back)], [(cw, third), (ccw, third)]]

    mixer_turns, up_turns, down_turns = turns_of(0, 1, 2), turns_of(3, 4, 5), turns_of(7, 6, 8)

    def wait_across(k, s):
        if shared(k):
            across(k, s, 1 - rep).wait_recv()

    def swap(src, dst, index):
        return pltpu.make_async_remote_copy(
            src_ref=src, dst_ref=dst, send_sem=tp_send.at[index], recv_sem=tp_recv.at[index],
            device_id={"tp": 1 - tp}, device_id_type=pl.DeviceIdType.MESH,
        )

    own = [
        (x_in, x_ref),
        (wg_in, wg.at[pl.ds(pl.multiple_of(fs * shard, TILE), shard), :]),
        (wi_in, wi.at[pl.ds(pl.multiple_of(fs * shard, TILE), shard), :]),
        (wo_in, wo.at[fs]),
        (wu_in, wu.at[pl.ds(pl.multiple_of(fs * shard, TILE), shard), :]),
        (wd_in, wd.at[fs]),
        (mgain_in, mgain_ref),
        (shift_in, shift_ref),
        (taps_in, taps_ref),
        (rg_in, rg_ref),
        (ig_in, ig_ref),
        (sp_in, sp_ref),
        (fgain_in, fgain_ref),
        (lgain_in, lgain_ref),
    ]
    local = [pltpu.make_async_copy(a, b, local_sems.at[i]) for i, (a, b) in enumerate(own)]
    barrier = pltpu.get_barrier_semaphore()
    for device in ({"fs": right}, {"fs": left}, {"rep": 1 - rep}, {"tp": 1 - tp}):
        pl.semaphore_signal(barrier, inc=1, device_id=device, device_id_type=pl.DeviceIdType.MESH)
    for i in (1, 2, 3, 0, 4, 5, *range(6, len(own))):
        local[i].start()
    pl.semaphore_wait(barrier, 4)
    swap_x = swap(x_ref, other, 0)
    for k in range(3):
        local[1 + k].wait()
    for turns in mixer_turns:
        for make, k in turns:
            make(k, 0).start()
    local[0].wait()
    swap_x.start()
    for i in range(4, len(own)):
        local[i].wait()

    own_cols = pl.ds(pl.multiple_of(tp * half, 128), half)
    other_cols = pl.ds(pl.multiple_of((1 - tp) * half, 128), half)

    def norm_block(first, second, gain_ref, rows):
        a = first[rows, :].astype(F32)
        b = second[rows, :].astype(F32)
        mean = (jnp.sum(a * a, axis=1, keepdims=True) + jnp.sum(b * b, axis=1, keepdims=True)) / (2 * half)
        scale = lax.rsqrt(mean + epsilon)
        normed[rows, own_cols] = (a * scale * gain_ref[:, own_cols]).astype(BF16)
        normed[rows, other_cols] = (b * scale * gain_ref[:, other_cols]).astype(BF16)

    small = 64

    pieces = length // small
    share = -(-pieces // (n - 2))

    @pl.loop(0, n - 2)
    def _(s):
        for turns in mixer_turns:
            service(turns, s, False)
        pl.when(s == 0)(swap_x.wait)

        @pl.when(s == n - 3)
        def _():
            for make, k in up_turns[0] + up_turns[1]:
                make(k, 0).start()

        for piece in range(share):
            i = s * share + piece

            @pl.when(i < pieces)
            def _():
                norm_block(x_ref, other, mgain_ref, pl.ds(pl.multiple_of(i * small, small), small))

    begin(ups[-1])
    for turns in mixer_turns:
        service(turns, n - 2, True)

    lead = n - 2

    def tick(t, j):
        pl.when(t < n - 1)(lambda: service(up_turns[j], t, None))

        if j == 2:

            @pl.when(t == n - 4)
            def _():
                for make, k in down_turns[0]:
                    make(k, 0).start()

            @pl.when(t == n - 3)
            def _():
                for make, k in down_turns[1]:
                    make(k, 0).start()
                begin(downs[2])

        pl.when(t >= lead)(lambda: service(down_turns[j], t - lead, None))

    for j in range(3):
        tick(0, j)

    @pl.loop(0, n - 1)
    def _(s):
        for k in range(3):
            wait_across(k, s)

    front[pl.ds(0, 8), :] = jnp.zeros((8, channels), F32)
    carry[...] = jnp.zeros_like(carry)
    decay_param = sp_ref[...]
    rate = rate_scale * (jnp.maximum(-decay_param, 0.0) + jnp.log1p(jnp.exp(-jnp.abs(decay_param))))
    num_taps = taps_ref.shape[0]
    groups = rg_ref.shape[0]
    block = rg_ref.shape[1]
    @pl.loop(0, blocks)
    def _(i):
        rows = pl.ds(pl.multiple_of(i * ROWS, ROWS), ROWS)
        tick(i + 1, 0)
        cols = normed[rows, :]
        front[pl.ds(8, ROWS), :] = jnp.dot(cols, wi[...], preferred_element_type=F32).astype(BF16).astype(F32)
        gate = jnp.dot(cols, wg[...], preferred_element_type=F32).astype(BF16)
        shift = jnp.transpose(jnp.broadcast_to(shift_ref[:, rows], (128, ROWS)))[:, :1]
        for g in range(groups):
            if g == 1:
                tick(i + 1, 1)
            ch = slice(g * block, (g + 1) * block)
            window = front[:, ch]
            filtered = jnp.zeros((ROWS, block), F32)
            for tap in range(num_taps):
                back = num_taps - 1 - tap
                moved = window if back == 0 else pltpu.roll(window, back, 0)
                filtered = filtered + moved[8:] * taps_ref[tap : tap + 1, ch]
            filtered = filtered.astype(BF16)
            recur = jax.nn.sigmoid(jnp.dot(filtered, rg_ref[g], preferred_element_type=F32))
            inlet = jax.nn.sigmoid(jnp.dot(filtered, ig_ref[g], preferred_element_type=F32))
            log_decay = shift - recur * rate[:, ch]
            a = jnp.exp(log_decay)
            b = jnp.sqrt(expm1_neg(2.0 * log_decay)) * inlet * filtered.astype(F32)
            a = a.reshape(ROWS // 8, 8, block)
            b = b.reshape(ROWS // 8, 8, block)
            at = lax.broadcasted_iota(jnp.int32, (ROWS // 8, 8, block), 1)
            for back in (1, 2, 4):
                keep = at >= back
                b = jnp.where(keep, a * pltpu.roll(b, back, 1) + b, b)
                a = jnp.where(keep, a * pltpu.roll(a, back, 1), a)
            scan_a[:, ch] = a.reshape(ROWS, block)
            scan_b[:, ch] = b.reshape(ROWS, block)
        front[pl.ds(0, 8), :] = front[pl.ds(ROWS, 8), :]

        def step_scan(t, h):
            at = pl.ds(pl.multiple_of(t * 8, 8), 8)
            states = scan_a[at, :] * h + scan_b[at, :]
            scan_b[at, :] = states
            return jnp.broadcast_to(states[7:8, :], states.shape)

        carry[...] = lax.fori_loop(0, ROWS // 8, step_scan, carry[...], unroll=4)
        tick(i + 1, 2)
        mixed = (scan_b[...] * jax.nn.gelu(gate.astype(F32), approximate=True)).astype(BF16)
        for j in range(half_n):
            to = pl.ds(j * width, width)
            part[1, rows, to] = jnp.dot(mixed, wo[(1 - tp) * half_n + j], preferred_element_type=F32).astype(BF16)
        swap(part.at[1, rows, :], prec.at[rows, :], 1 + i).start()
        for j in range(half_n):
            to = pl.ds(j * width, width)
            part[0, rows, to] = jnp.dot(mixed, wo[tp * half_n + j], preferred_element_type=F32).astype(BF16)

    tick(blocks + 1, 0)

    @pl.loop(0, blocks)
    def _(i):
        rows = pl.ds(pl.multiple_of(i * ROWS, ROWS), ROWS)
        swap(part.at[1, rows, :], prec.at[rows, :], 1 + i).wait()
        mid[rows, :] = (
            x_ref[rows, :].astype(F32) + (part[0, rows, :].astype(F32) + prec[rows, :].astype(F32))
        ).astype(BF16)
        swap(mid.at[rows, :], mid_other.at[rows, :], 1 + blocks + i).start()

    tick(blocks + 1, 1)

    @pl.loop(0, blocks)
    def _(i):
        rows = pl.ds(pl.multiple_of(i * ROWS, ROWS), ROWS)
        swap(mid.at[rows, :], mid_other.at[rows, :], 1 + blocks + i).wait()

    tick(blocks + 1, 2)

    for part_of in range(2):

        @pl.loop(part_of * (pieces // 2), (part_of + 1) * (pieces // 2))
        def _(i):
            norm_block(mid, mid_other, fgain_ref, pl.ds(pl.multiple_of(i * small, small), small))

        tick(blocks + 2, part_of)

    tick(blocks + 2, 2)
    for t in range(blocks + 3, n + 1):
        for j in range(3):
            tick(t, j)

    @pl.loop(0, n - 1)
    def _(s):
        for k in ups:
            wait_across(k, s)

    up_cols = min(512, hidden)
    @pl.loop(0, hidden // up_cols)
    def _(c):
        to = pl.ds(pl.multiple_of(c * up_cols, up_cols), up_cols)

        @pl.loop(0, blocks)
        def _(i):
            rows = pl.ds(pl.multiple_of(i * ROWS, ROWS), ROWS)
            up = jnp.maximum(jnp.dot(normed[rows, :], wu[:, to], preferred_element_type=F32), 0.0)
            act[rows, to] = (up * up).astype(BF16)

        for j in range(3):
            pl.when(c == j)(functools.partial(tick, n + 1, j))

    tick(n + 2, 0)

    def place(owner, i):
        column = lax.rem(owner, half_n)
        slot = lax.rem(owner // half_n + tp, 2)
        rows = pl.ds(pl.multiple_of(i * ROWS, ROWS), ROWS)
        to = pl.ds(pl.multiple_of(column * width, 128), width)
        return column, slot, rows, to

    def back_swap(column, i):
        _, _, rows, to = place(column, i)
        return swap(part.at[1, rows, to], prec.at[rows, to], 1 + 2 * blocks + column * blocks + i)

    def write(column, i):
        _, _, rows, to = place(column, i)
        return pltpu.make_async_copy(other.at[rows, to], out_ref.at[rows, to], out_sems.at[column * blocks + i])

    def down_rows(owner, i):
        column, slot, rows, to = place(owner, i)
        part[slot, rows, to] = jnp.dot(act[rows, :], wd[owner], preferred_element_type=F32).astype(BF16)
        pl.when(slot == 1)(lambda: back_swap(column, i).start())

    def early_rows(e, owner, i):
        rows = pl.ds(pl.multiple_of(i * ROWS, ROWS), ROWS)
        take = pl.ds((1 - e) * half_d, half_d)
        acc[e, rows, :] = jnp.dot(act[rows, take], wd[owner, take, :], preferred_element_type=F32)

    def late_rows(e, owner, i):
        column, slot, rows, to = place(owner, i)
        take = pl.ds(e * half_d, half_d)
        rest = jnp.dot(act[rows, take], wd[owner, take, :], preferred_element_type=F32)
        part[slot, rows, to] = (acc[e, rows, :] + rest).astype(BF16)
        pl.when(slot == 1)(lambda: back_swap(column, i).start())

    def total_rows(owner, i):
        column, slot, rows, to = place(owner, i)

        @pl.when(slot == 0)
        def _():
            back_swap(column, i).wait_recv()
            total = mid[rows, to].astype(F32) + (part[0, rows, to].astype(F32) + prec[rows, to].astype(F32))
            other[rows, to] = (total * lgain_ref[:, to]).astype(BF16)
            squares = total * total
            sq_send[rows, :] += sum(squares[:, at : at + 128] for at in range(0, width, 128))
            write(column, i).start()

    def over_rows(*makes):
        @pl.loop(0, blocks)
        def _(i):
            for make, owner in makes:
                make(owner, i)

    order = [ring_to_fs(pos + ahead) for ahead in [0, half_n]]
    for s in range(half_n, n - 1):
        order += [ring_to_fs(pos - s - 1), ring_to_fs(pos + s + 1)]
    sq_send[...] = jnp.zeros_like(sq_send)
    over_rows((down_rows, order[0]))
    for at in range(3 * n + 7, 3 * (lead + half_n + 1)):
        tick(at // 3, at % 3)
    for s in range(half_n):
        for k in downs:
            wait_across(k, s)
    over_rows((down_rows, order[1]), (total_rows, order[0]))
    for e in range(2):
        over_rows((functools.partial(early_rows, e), order[e - 2]))
    for s in range(half_n, n - 2):
        at = 2 * (s - half_n + 1)
        tick(lead + s + 1, 0)
        for k in downs:
            wait_across(k, s)
        over_rows((down_rows, order[at]), (total_rows, order[at - 1]))
        tick(lead + s + 1, 1)
        over_rows((down_rows, order[at + 1]), (total_rows, order[at]))
        tick(lead + s + 1, 2)
    for k in downs:
        wait_across(k, n - 2)

    def swap_sq(i):
        rows = pl.ds(pl.multiple_of(i * ROWS, ROWS), ROWS)
        return swap(sq_send.at[rows, :], sq_recv.at[rows, :], 1 + 2 * blocks + half_n * blocks + i)

    def settle(i):
        total_rows(order[-2], i)
        total_rows(order[-1], i)
        swap_sq(i).start()

    @pl.loop(0, blocks)
    def _(i):
        late_rows(0, order[-2], i)
        late_rows(1, order[-1], i)
        total_rows(order[-3], i)
        pl.when(i > 0)(lambda: settle(i - 1))

    settle(blocks - 1)

    def write_scale(i):
        rows = pl.ds(pl.multiple_of(i * ROWS, ROWS), ROWS)
        return pltpu.make_async_copy(scales.at[rows, :], scale_ref.at[rows, :], out_sems.at[half_n * blocks + i])

    @pl.loop(0, blocks)
    def _(i):
        swap_sq(i).wait()
        rows = pl.ds(pl.multiple_of(i * ROWS, ROWS), ROWS)
        squares = jnp.sum(sq_send[rows, :] + sq_recv[rows, :], axis=1, keepdims=True)
        scales[rows, :] = jnp.broadcast_to(lax.rsqrt(squares / (2 * half) + epsilon), (ROWS, 128))
        write_scale(i).start()

    @pl.loop(0, n - 1)
    def _(s):
        for k in range(len(views)):
            cw(k, s).wait_send()
            ccw(k, s).wait_send()
            if shared(k):
                across(k, s, rep).wait_send()

    @pl.loop(0, blocks)
    def _(i):
        for j in range(half_n):
            back_swap(j, i).wait_send()
            write(j, i).wait()
        write_scale(i).wait()


CHUNKS = 8


def closing_kernel(total_in, scale_in, out_ref, total, scale, result, sems):
    rows = total.shape[0] // CHUNKS

    def copies(i):
        at = pl.ds(i * rows, rows)
        return (
            pltpu.make_async_copy(total_in.at[at, :], total.at[at, :], sems.at[0, i]),
            pltpu.make_async_copy(scale_in.at[at, :], scale.at[at, :], sems.at[1, i]),
            pltpu.make_async_copy(result.at[at, :], out_ref.at[at, :], sems.at[2, i]),
        )

    for i in range(CHUNKS):
        first, second, _ = copies(i)
        first.start()
        second.start()
    for i in range(CHUNKS):
        first, second, third = copies(i)
        first.wait()
        second.wait()
        at = pl.ds(i * rows, rows)
        result[at, :] = (total[at, :].astype(F32) * scale[at, :1]).astype(BF16)
        third.start()
    for i in range(CHUNKS):
        copies(i)[2].wait()


def fused(n, stream_in, decay_shift, mixer_gain, gate_weight, input_weight, filter_taps, recur_gate,
          inlet_gate, decay_param, mixer_out, feedforward_gain, up_weight, down_weight, final_gain):
    _, length, half = stream_in.shape
    shard, channels = gate_weight.shape
    hidden = up_weight.shape[1]
    width = down_weight.shape[1]
    model = shard * n
    blocks = length // ROWS
    half_n = n // 2
    vmem = pl.BlockSpec(memory_space=pltpu.VMEM)
    hbm = pl.BlockSpec(memory_space=pl.ANY)
    swaps = 1 + 2 * blocks + half_n * blocks + blocks
    total, scale = pl.pallas_call(
        functools.partial(layer_kernel, n),
        out_shape=(jax.ShapeDtypeStruct((length, half), BF16), jax.ShapeDtypeStruct((length, 128), F32)),
        in_specs=[hbm] * 14,
        out_specs=(hbm, hbm),
        scratch_shapes=[
            pltpu.VMEM((1, length), F32),
            pltpu.VMEM((1, model), F32),
            pltpu.VMEM(filter_taps.shape, F32),
            pltpu.VMEM(recur_gate.shape, BF16),
            pltpu.VMEM(inlet_gate.shape, BF16),
            pltpu.VMEM((1, channels), F32),
            pltpu.VMEM((1, model), F32),
            pltpu.VMEM((1, half), F32),
            pltpu.VMEM((length, half), BF16),
            pltpu.VMEM((model, channels), BF16),
            pltpu.VMEM((model, channels), BF16),
            pltpu.VMEM((n, channels, width), BF16),
            pltpu.VMEM((model, hidden), BF16),
            pltpu.VMEM((n, hidden, width), BF16),
            pltpu.VMEM((length, half), BF16),
            pltpu.VMEM((length, model), BF16),
            pltpu.VMEM((8 + ROWS, channels), F32),
            pltpu.VMEM((8, channels), F32),
            pltpu.VMEM((ROWS, channels), F32),
            pltpu.VMEM((ROWS, channels), F32),
            pltpu.VMEM((2, length, half), BF16),
            pltpu.VMEM((length, half), BF16),
            pltpu.VMEM((length, half), BF16),
            pltpu.VMEM((length, half), BF16),
            pltpu.VMEM((length, hidden), BF16),
            pltpu.VMEM((length, 128), F32),
            pltpu.VMEM((length, 128), F32),
            pltpu.VMEM((2, length, width), F32),
            pltpu.VMEM((length, 128), F32),
            pltpu.SemaphoreType.DMA((14,)),
            pltpu.SemaphoreType.DMA((9, 3, n - 1)),
            pltpu.SemaphoreType.DMA((9, 3, n - 1)),
            pltpu.SemaphoreType.DMA((swaps,)),
            pltpu.SemaphoreType.DMA((swaps,)),
            pltpu.SemaphoreType.DMA((half_n * blocks + blocks,)),
        ],
        compiler_params=pltpu.CompilerParams(
            collective_id=0, has_side_effects=True, vmem_limit_bytes=67043328
        ),
        name="gated_layer",
    )(
        stream_in.reshape(length, half),
        decay_shift,
        mixer_gain.reshape(1, -1),
        gate_weight,
        input_weight,
        filter_taps,
        recur_gate,
        inlet_gate,
        decay_param.reshape(1, -1),
        mixer_out,
        feedforward_gain.reshape(1, -1),
        up_weight,
        down_weight,
        final_gain.reshape(1, -1),
    )
    out = pl.pallas_call(
        closing_kernel,
        out_shape=jax.ShapeDtypeStruct((length, half), BF16),
        in_specs=[hbm, hbm],
        out_specs=hbm,
        scratch_shapes=[
            pltpu.VMEM((length, half), BF16),
            pltpu.VMEM((length, 128), F32),
            pltpu.VMEM((length, half), BF16),
            pltpu.SemaphoreType.DMA((3, CHUNKS)),
        ],
        name="closing",
    )(total, scale)
    return out.reshape(1, length, half)


def fits(mesh, n, args):
    num_seq, length, half = args[0].shape
    width = args[9].shape[1]
    shard = args[3].shape[0]
    return (
        mesh.shape["rep"] == 2 and mesh.shape["tp"] == 2 and n % 8 == 0 and num_seq == 1
        and width % 128 == 0 and args[11].shape[1] % 1024 == 0 and length == 4 * ROWS and shard >= 3 * TILE and length % ROWS == 0
    )


def local_for(mesh):
    n = mesh.shape["fs"]

    def local(*args):
        if fits(mesh, n, args):
            return fused(n, *args)
        return plain(*args)

    return local


def solution(mesh):
    return jax.shard_map(
        local_for(mesh),
        mesh=mesh,
        in_specs=(
            P(("rep", "fs"), None, "tp"),
            P(("rep", "fs"), None),
            P(),
            P("fs", "tp"),
            P("fs", "tp"),
            P(None, "tp"),
            P("tp", None, None),
            P("tp", None, None),
            P("tp"),
            P("tp", "fs"),
            P(),
            P("fs", "tp"),
            P("tp", "fs"),
            P("tp"),
        ),
        out_specs=P(("rep", "fs"), None, "tp"),
        check_vma=False,
    )
```

```python
import functools

import jax
import jax.numpy as jnp
from jax import lax
from jax.experimental import pallas as pl
from jax.experimental.pallas import tpu as pltpu
from jax.sharding import PartitionSpec as P

D = 2048


epsilon = 1e-06
rate_scale = 8.0


def norm_rows(values, row_gain):
    mean_sq = jnp.mean(values * values, axis=-1, keepdims=True)
    return values * lax.rsqrt(mean_sq + epsilon) * row_gain


def combine(earlier, later):
    return (earlier[0] * later[0], later[0] * earlier[1] + later[1])


def plain(
    stream_in,
    decay_shift,
    mixer_gain,
    gate_weight,
    input_weight,
    filter_taps,
    recur_gate,
    inlet_gate,
    decay_param,
    mixer_out,
    feedforward_gain,
    up_weight,
    down_weight,
    final_gain,
):
    num_seq, length, half_width = stream_in.shape
    whole = lax.all_gather(stream_in, "tp", axis=2, tiled=True)
    flat_rows = num_seq * length
    normed = norm_rows(whole.reshape(flat_rows, -1).astype(jnp.float32), mixer_gain).astype(
        jnp.bfloat16
    )
    channels = gate_weight.shape[1]
    columns = normed
    gate_logits = jnp.dot(
        columns,
        lax.all_gather(gate_weight, "fs", axis=0, tiled=True),
        preferred_element_type=jnp.float32,
    )
    input_pre = jnp.dot(
        columns,
        lax.all_gather(input_weight, "fs", axis=0, tiled=True),
        preferred_element_type=jnp.float32,
    )
    gate_logits = gate_logits.astype(jnp.bfloat16)
    input_pre = input_pre.astype(jnp.bfloat16)
    branch = jax.nn.gelu(gate_logits.astype(jnp.float32), approximate=True)
    num_taps = filter_taps.shape[0]
    extended_front = jnp.pad(
        input_pre.astype(jnp.float32).reshape(num_seq, length, channels),
        ((0, 0), (num_taps - 1, 0), (0, 0)),
    )
    filtered = jnp.zeros((num_seq, length, channels), jnp.float32)
    for offset in range(num_taps):
        filtered = (
            filtered
            + extended_front[:, offset : offset + length] * filter_taps[offset][None, None, :]
        )
    filtered = filtered.astype(jnp.bfloat16).reshape(flat_rows, channels)
    num_blocks = recur_gate.shape[0]
    grouped = filtered.reshape(flat_rows, num_blocks, recur_gate.shape[1])
    recur = jax.nn.sigmoid(
        jnp.einsum("lni,nij->lnj", grouped, recur_gate, preferred_element_type=jnp.float32).reshape(
            flat_rows, channels
        )
    )
    inlet = jax.nn.sigmoid(
        jnp.einsum("lni,nij->lnj", grouped, inlet_gate, preferred_element_type=jnp.float32).reshape(
            flat_rows, channels
        )
    )
    logarithm_decay = (
        -rate_scale * recur * jax.nn.softplus(-decay_param)[None, :]
        + decay_shift.reshape(flat_rows)[:, None]
    )
    decay = jnp.exp(logarithm_decay).reshape(num_seq, length, channels)
    drive = (
        jnp.sqrt(-jnp.expm1(2.0 * logarithm_decay)) * inlet * filtered.astype(jnp.float32)
    ).reshape(num_seq, length, channels)
    states = lax.associative_scan(combine, (decay, drive), axis=1)[1]
    mixed = (states.reshape(flat_rows, channels) * branch).astype(jnp.bfloat16)
    mixer_terms = (
        jnp.dot(
            mixed,
            lax.all_gather(mixer_out, "fs", axis=1, tiled=True),
            preferred_element_type=jnp.float32,
        )
        .astype(jnp.bfloat16)
        .astype(jnp.float32)
    )
    mixer_sum = lax.psum_scatter(
        mixer_terms.astype(jnp.bfloat16), "tp", scatter_dimension=1, tiled=True
    ).astype(jnp.float32)
    stream_mid = (stream_in.reshape(flat_rows, half_width).astype(jnp.float32) + mixer_sum).astype(
        jnp.bfloat16
    )
    stream_whole = lax.all_gather(stream_mid, "tp", axis=1, tiled=True)
    normed_mid = norm_rows(stream_whole.astype(jnp.float32), feedforward_gain).astype(jnp.bfloat16)
    columns = normed_mid
    up_proj = jnp.dot(
        columns,
        lax.all_gather(up_weight, "fs", axis=0, tiled=True),
        preferred_element_type=jnp.float32,
    )
    activated = jnp.square(jax.nn.relu(up_proj)).astype(jnp.bfloat16)
    ffn_terms = (
        jnp.dot(
            activated,
            lax.all_gather(down_weight, "fs", axis=1, tiled=True),
            preferred_element_type=jnp.float32,
        )
        .astype(jnp.bfloat16)
        .astype(jnp.float32)
    )
    ffn_sum = lax.psum_scatter(
        ffn_terms.astype(jnp.bfloat16), "tp", scatter_dimension=1, tiled=True
    ).astype(jnp.float32)
    total = stream_mid.astype(jnp.float32) + ffn_sum
    squares_sum = lax.psum(jnp.sum(total * total, axis=1), "tp")
    layer_out = total * lax.rsqrt(squares_sum / D + epsilon)[:, None] * final_gain[None, :]
    return layer_out.astype(jnp.bfloat16).reshape(num_seq, length, half_width)


F32 = jnp.float32
BF16 = jnp.bfloat16
TILE = 16
FORE, BACK, BOTH = range(3)
ROWS = 256


def split_rows(rows, up):
    third = rows // 3 // TILE * TILE + (TILE if up else 0)
    return rows - 2 * third, third


def expm1_neg(v):
    series = -v * (1.0 + v * (1 / 2) * (1.0 + v * (1 / 3) * (1.0 + v * (1 / 4) * (1.0 + v * (1 / 5) * (1.0 + v * (1 / 6))))))
    return jnp.where(v > -0.25, series, 1.0 - jnp.exp(v))


def layer_kernel(
    n,
    x_in, shift_in, mgain_in, wg_in, wi_in, taps_in, rg_in, ig_in, sp_in, wo_in,
    fgain_in, wu_in, wd_in, lgain_in,
    out_ref, scale_ref,
    shift_ref, mgain_ref, taps_ref, rg_ref, ig_ref, sp_ref, fgain_ref, lgain_ref,
    x_ref, wg, wi, wo, wu, wd, other, normed, front, carry, scan_a, scan_b, part, prec, mid, mid_other,
    act, sq_send, sq_recv, acc, scales,
    local_sems, send_sems, recv_sems, tp_send, tp_recv, out_sems,
):
    rep, fs, tp = lax.axis_index("rep"), lax.axis_index("fs"), lax.axis_index("tp")
    half_n = n // 2
    length, half = x_in.shape
    channels = wg.shape[1]
    width = wd.shape[2]
    shard = wg_in.shape[0]
    hidden = wu.shape[1]
    blocks = length // ROWS

    def ring_to_fs(p):
        p = lax.rem(p + 2 * n, n)
        return jnp.where(p < half_n, 2 * p, 2 * (n - 1 - p) + 1)

    odd = lax.rem(fs, 2)
    pos = (1 - odd) * (fs // 2) + odd * (n - 1 - fs // 2)
    right, left = ring_to_fs(pos + 1), ring_to_fs(pos - 1)

    def by_row(dst, lo, cols):
        def view(owner, off, size):
            return dst.at[pl.ds(pl.multiple_of(owner * shard + off, TILE), size), pl.ds(lo, cols)]
        return view

    def by_owner(dst, lo):
        def view(owner, off, size):
            return dst.at[owner, pl.ds(pl.multiple_of(lo + off, TILE), size), :]
        return view

    rows_o, rows_d = wo.shape[1], wd.shape[1]
    def plain_split(rows, up):
        p, q = split_rows(rows, up)
        return (0, p), (p, q)

    quarter = hidden // 4
    half_d = rows_d // 2
    private, last = rows_d // 8, rows_d // 16
    common = half_d - 2 * private - last
    views = [
        (by_row(wg, 0, channels), BACK, plain_split(shard, True)),
        (by_row(wi, 0, channels), FORE, plain_split(shard, True)),
        (by_owner(wo, 0), FORE, plain_split(rows_o, True)),
        (by_row(wu, 0, quarter), BACK, plain_split(shard, True)),
        (by_row(wu, quarter, 2 * quarter), FORE, plain_split(shard, True)),
        (by_row(wu, 3 * quarter, quarter), BACK, plain_split(shard, True)),
        (by_owner(wd, 0), FORE, ((0, common), (half_d, private))),
        (by_owner(wd, 0), BACK, ((half_d + 2 * private, common), (common + last, private))),
        (by_owner(wd, 0), BOTH, ((common, last), (rows_d - last, last))),
    ]
    ups = range(3, 6)
    downs = range(6, 9)

    def remote(view, k, lane, s, device):
        return pltpu.make_async_remote_copy(
            src_ref=view, dst_ref=view, send_sem=send_sems.at[k, lane, lax.rem(s, 2)],
            recv_sem=recv_sems.at[k, lane, s], device_id=device,
            device_id_type=pl.DeviceIdType.MESH,
        )

    def cw(k, s, shift=0):
        view, role, (whole, (lo, size)) = views[k]
        at = (lo + rep * size, size) if role == BACK else whole
        return remote(view(ring_to_fs(pos - s - shift), *at), k, 0, s, {"fs": right})

    def ccw(k, s, shift=0):
        view, role, (whole, (lo, size)) = views[k]
        at = whole if role == BACK else (lo + rep * size if role == FORE else lo, size)
        return remote(view(ring_to_fs(pos + s + shift), *at), k, 1, s, {"fs": left})

    def across(k, s, side):
        view, role, (_, (lo, size)) = views[k]
        owner = pos + s + 1 if role == FORE else pos - s - 1
        return remote(view(ring_to_fs(owner), lo + side * size, size), k, 2, s, {"rep": 1 - rep})

    def shared(k):
        return views[k][1] != BOTH

    def begin(k):
        cw(k, 0).start()
        ccw(k, 0).start()

    def launch(make, k, s, *side):
        pl.when(s >= 2)(lambda: make(k, s - 2, *side).wait_send())
        make(k, s, *side).start()

    def service(turns, s, last):
        for make, k in turns:
            make(k, s, 1).wait_recv()
            if last is None:
                pl.when(s + 1 < n - 1)(functools.partial(launch, make, k, s + 1))
            elif not last:
                launch(make, k, s + 1)
            if views[k][1] == (BACK if make is cw else FORE):
                launch(across, k, s, rep)

    def turns_of(back, fore, third):
        return [[(cw, back), (ccw, fore)], [(cw, fore), (ccw, back)], [(cw, third), (ccw, third)]]

    mixer_turns, up_turns, down_turns = turns_of(0, 1, 2), turns_of(3, 4, 5), turns_of(7, 6, 8)

    def wait_across(k, s):
        if shared(k):
            across(k, s, 1 - rep).wait_recv()

    def swap(src, dst, index):
        return pltpu.make_async_remote_copy(
            src_ref=src, dst_ref=dst, send_sem=tp_send.at[index], recv_sem=tp_recv.at[index],
            device_id={"tp": 1 - tp}, device_id_type=pl.DeviceIdType.MESH,
        )

    own = [
        (x_in, x_ref),
        (wg_in, wg.at[pl.ds(pl.multiple_of(fs * shard, TILE), shard), :]),
        (wi_in, wi.at[pl.ds(pl.multiple_of(fs * shard, TILE), shard), :]),
        (wo_in, wo.at[fs]),
        (wu_in, wu.at[pl.ds(pl.multiple_of(fs * shard, TILE), shard), :]),
        (wd_in, wd.at[fs]),
        (mgain_in, mgain_ref),
        (shift_in, shift_ref),
        (taps_in, taps_ref),
        (rg_in, rg_ref),
        (ig_in, ig_ref),
        (sp_in, sp_ref),
        (fgain_in, fgain_ref),
        (lgain_in, lgain_ref),
    ]
    local = [pltpu.make_async_copy(a, b, local_sems.at[i]) for i, (a, b) in enumerate(own)]
    barrier = pltpu.get_barrier_semaphore()
    for device in ({"fs": right}, {"fs": left}, {"rep": 1 - rep}, {"tp": 1 - tp}):
        pl.semaphore_signal(barrier, inc=1, device_id=device, device_id_type=pl.DeviceIdType.MESH)
    for i in (1, 2, 3, 0, 4, 5, *range(6, len(own))):
        local[i].start()
    pl.semaphore_wait(barrier, 4)
    swap_x = swap(x_ref, other, 0)
    for k in range(3):
        local[1 + k].wait()
    for turns in mixer_turns:
        for make, k in turns:
            make(k, 0).start()
    local[0].wait()
    swap_x.start()
    for i in range(4, len(own)):
        local[i].wait()

    own_cols = pl.ds(pl.multiple_of(tp * half, 128), half)
    other_cols = pl.ds(pl.multiple_of((1 - tp) * half, 128), half)

    def norm_block(first, second, gain_ref, rows):
        a = first[rows, :].astype(F32)
        b = second[rows, :].astype(F32)
        mean = (jnp.sum(a * a, axis=1, keepdims=True) + jnp.sum(b * b, axis=1, keepdims=True)) / (2 * half)
        scale = lax.rsqrt(mean + epsilon)
        normed[rows, own_cols] = (a * scale * gain_ref[:, own_cols]).astype(BF16)
        normed[rows, other_cols] = (b * scale * gain_ref[:, other_cols]).astype(BF16)

    small = 64

    pieces = length // small
    share = -(-pieces // (n - 2))

    @pl.loop(0, n - 2)
    def _(s):
        for turns in mixer_turns:
            service(turns, s, False)
        pl.when(s == 0)(swap_x.wait)

        @pl.when(s == n - 3)
        def _():
            for make, k in up_turns[0] + up_turns[1]:
                make(k, 0).start()

        for piece in range(share):
            i = s * share + piece

            @pl.when(i < pieces)
            def _():
                norm_block(x_ref, other, mgain_ref, pl.ds(pl.multiple_of(i * small, small), small))

    begin(ups[-1])
    for turns in mixer_turns:
        service(turns, n - 2, True)

    lead = n - 2

    def tick(t, j):
        pl.when(t < n - 1)(lambda: service(up_turns[j], t, None))

        if j == 2:

            @pl.when(t == n - 4)
            def _():
                for make, k in down_turns[0]:
                    make(k, 0).start()

            @pl.when(t == n - 3)
            def _():
                for make, k in down_turns[1]:
                    make(k, 0).start()
                begin(downs[2])

        pl.when(t >= lead)(lambda: service(down_turns[j], t - lead, None))

    for j in range(3):
        tick(0, j)

    @pl.loop(0, n - 1)
    def _(s):
        for k in range(3):
            wait_across(k, s)

    front[pl.ds(0, 8), :] = jnp.zeros((8, channels), F32)
    carry[...] = jnp.zeros_like(carry)
    decay_param = sp_ref[...]
    rate = rate_scale * (jnp.maximum(-decay_param, 0.0) + jnp.log1p(jnp.exp(-jnp.abs(decay_param))))
    num_taps = taps_ref.shape[0]
    groups = rg_ref.shape[0]
    block = rg_ref.shape[1]
    @pl.loop(0, blocks)
    def _(i):
        rows = pl.ds(pl.multiple_of(i * ROWS, ROWS), ROWS)
        tick(i + 1, 0)
        cols = normed[rows, :]
        front[pl.ds(8, ROWS), :] = jnp.dot(cols, wi[...], preferred_element_type=F32).astype(BF16).astype(F32)
        gate = jnp.dot(cols, wg[...], preferred_element_type=F32).astype(BF16)
        shift = jnp.transpose(jnp.broadcast_to(shift_ref[:, rows], (128, ROWS)))[:, :1]
        for g in range(groups):
            if g == 1:
                tick(i + 1, 1)
            ch = slice(g * block, (g + 1) * block)
            window = front[:, ch]
            filtered = jnp.zeros((ROWS, block), F32)
            for tap in range(num_taps):
                back = num_taps - 1 - tap
                moved = window if back == 0 else pltpu.roll(window, back, 0)
                filtered = filtered + moved[8:] * taps_ref[tap : tap + 1, ch]
            filtered = filtered.astype(BF16)
            recur = jax.nn.sigmoid(jnp.dot(filtered, rg_ref[g], preferred_element_type=F32))
            inlet = jax.nn.sigmoid(jnp.dot(filtered, ig_ref[g], preferred_element_type=F32))
            log_decay = shift - recur * rate[:, ch]
            a = jnp.exp(log_decay)
            b = jnp.sqrt(expm1_neg(2.0 * log_decay)) * inlet * filtered.astype(F32)
            a = a.reshape(ROWS // 8, 8, block)
            b = b.reshape(ROWS // 8, 8, block)
            at = lax.broadcasted_iota(jnp.int32, (ROWS // 8, 8, block), 1)
            for back in (1, 2, 4):
                keep = at >= back
                b = jnp.where(keep, a * pltpu.roll(b, back, 1) + b, b)
                a = jnp.where(keep, a * pltpu.roll(a, back, 1), a)
            scan_a[:, ch] = a.reshape(ROWS, block)
            scan_b[:, ch] = b.reshape(ROWS, block)
        front[pl.ds(0, 8), :] = front[pl.ds(ROWS, 8), :]

        def step_scan(t, h):
            at = pl.ds(pl.multiple_of(t * 8, 8), 8)
            states = scan_a[at, :] * h + scan_b[at, :]
            scan_b[at, :] = states
            return jnp.broadcast_to(states[7:8, :], states.shape)

        carry[...] = lax.fori_loop(0, ROWS // 8, step_scan, carry[...], unroll=4)
        tick(i + 1, 2)
        mixed = (scan_b[...] * jax.nn.gelu(gate.astype(F32), approximate=True)).astype(BF16)
        for j in range(half_n):
            to = pl.ds(j * width, width)
            part[1, rows, to] = jnp.dot(mixed, wo[(1 - tp) * half_n + j], preferred_element_type=F32).astype(BF16)
        swap(part.at[1, rows, :], prec.at[rows, :], 1 + i).start()
        for j in range(half_n):
            to = pl.ds(j * width, width)
            part[0, rows, to] = jnp.dot(mixed, wo[tp * half_n + j], preferred_element_type=F32).astype(BF16)

    tick(blocks + 1, 0)

    @pl.loop(0, blocks)
    def _(i):
        rows = pl.ds(pl.multiple_of(i * ROWS, ROWS), ROWS)
        swap(part.at[1, rows, :], prec.at[rows, :], 1 + i).wait()
        mid[rows, :] = (
            x_ref[rows, :].astype(F32) + (part[0, rows, :].astype(F32) + prec[rows, :].astype(F32))
        ).astype(BF16)
        swap(mid.at[rows, :], mid_other.at[rows, :], 1 + blocks + i).start()

    tick(blocks + 1, 1)

    @pl.loop(0, blocks)
    def _(i):
        rows = pl.ds(pl.multiple_of(i * ROWS, ROWS), ROWS)
        swap(mid.at[rows, :], mid_other.at[rows, :], 1 + blocks + i).wait()

    tick(blocks + 1, 2)

    for part_of in range(2):

        @pl.loop(part_of * (pieces // 2), (part_of + 1) * (pieces // 2))
        def _(i):
            norm_block(mid, mid_other, fgain_ref, pl.ds(pl.multiple_of(i * small, small), small))

        tick(blocks + 2, part_of)

    tick(blocks + 2, 2)
    for t in range(blocks + 3, n + 1):
        for j in range(3):
            tick(t, j)

    @pl.loop(0, n - 1)
    def _(s):
        for k in ups:
            wait_across(k, s)

    up_cols = min(512, hidden)
    @pl.loop(0, hidden // up_cols)
    def _(c):
        to = pl.ds(pl.multiple_of(c * up_cols, up_cols), up_cols)

        @pl.loop(0, blocks)
        def _(i):
            rows = pl.ds(pl.multiple_of(i * ROWS, ROWS), ROWS)
            up = jnp.maximum(jnp.dot(normed[rows, :], wu[:, to], preferred_element_type=F32), 0.0)
            act[rows, to] = (up * up).astype(BF16)

        for j in range(3):
            pl.when(c == j)(functools.partial(tick, n + 1, j))

    tick(n + 2, 0)

    def place(owner, i):
        column = lax.rem(owner, half_n)
        slot = lax.rem(owner // half_n + tp, 2)
        rows = pl.ds(pl.multiple_of(i * ROWS, ROWS), ROWS)
        to = pl.ds(pl.multiple_of(column * width, 128), width)
        return column, slot, rows, to

    def back_swap(column, i):
        _, _, rows, to = place(column, i)
        return swap(part.at[1, rows, to], prec.at[rows, to], 1 + 2 * blocks + column * blocks + i)

    def write(column, i):
        _, _, rows, to = place(column, i)
        return pltpu.make_async_copy(other.at[rows, to], out_ref.at[rows, to], out_sems.at[column * blocks + i])

    def down_rows(owner, i):
        column, slot, rows, to = place(owner, i)
        part[slot, rows, to] = jnp.dot(act[rows, :], wd[owner], preferred_element_type=F32).astype(BF16)
        pl.when(slot == 1)(lambda: back_swap(column, i).start())

    def early_rows(e, owner, i):
        rows = pl.ds(pl.multiple_of(i * ROWS, ROWS), ROWS)
        take = pl.ds((1 - e) * half_d, half_d)
        acc[e, rows, :] = jnp.dot(act[rows, take], wd[owner, take, :], preferred_element_type=F32)

    def late_rows(e, owner, i):
        column, slot, rows, to = place(owner, i)
        take = pl.ds(e * half_d, half_d)
        rest = jnp.dot(act[rows, take], wd[owner, take, :], preferred_element_type=F32)
        part[slot, rows, to] = (acc[e, rows, :] + rest).astype(BF16)
        pl.when(slot == 1)(lambda: back_swap(column, i).start())

    def total_rows(owner, i):
        column, slot, rows, to = place(owner, i)

        @pl.when(slot == 0)
        def _():
            back_swap(column, i).wait_recv()
            total = mid[rows, to].astype(F32) + (part[0, rows, to].astype(F32) + prec[rows, to].astype(F32))
            other[rows, to] = (total * lgain_ref[:, to]).astype(BF16)
            squares = total * total
            sq_send[rows, :] += sum(squares[:, at : at + 128] for at in range(0, width, 128))
            write(column, i).start()

    def over_rows(*makes):
        @pl.loop(0, blocks)
        def _(i):
            for make, owner in makes:
                make(owner, i)

    order = [ring_to_fs(pos + ahead) for ahead in [0, half_n]]
    for s in range(half_n, n - 1):
        order += [ring_to_fs(pos - s - 1), ring_to_fs(pos + s + 1)]
    sq_send[...] = jnp.zeros_like(sq_send)
    over_rows((down_rows, order[0]))
    for at in range(3 * n + 7, 3 * (lead + half_n + 1)):
        tick(at // 3, at % 3)
    for s in range(half_n):
        for k in downs:
            wait_across(k, s)
    over_rows((down_rows, order[1]), (total_rows, order[0]))
    for e in range(2):
        over_rows((functools.partial(early_rows, e), order[e - 2]))
    for s in range(half_n, n - 2):
        at = 2 * (s - half_n + 1)
        tick(lead + s + 1, 0)
        for k in downs:
            wait_across(k, s)
        over_rows((down_rows, order[at]), (total_rows, order[at - 1]))
        tick(lead + s + 1, 1)
        over_rows((down_rows, order[at + 1]), (total_rows, order[at]))
        tick(lead + s + 1, 2)
    wait_across(downs[1], n - 2)
    over_rows((functools.partial(late_rows, 0), order[-2]), (total_rows, order[-3]))
    wait_across(downs[0], n - 2)

    def swap_sq(i):
        rows = pl.ds(pl.multiple_of(i * ROWS, ROWS), ROWS)
        return swap(sq_send.at[rows, :], sq_recv.at[rows, :], 1 + 2 * blocks + half_n * blocks + i)

    def settle(i):
        total_rows(order[-2], i)
        total_rows(order[-1], i)
        swap_sq(i).start()

    @pl.loop(0, blocks)
    def _(i):
        late_rows(1, order[-1], i)
        pl.when(i > 0)(lambda: settle(i - 1))

    settle(blocks - 1)

    def write_scale(i):
        rows = pl.ds(pl.multiple_of(i * ROWS, ROWS), ROWS)
        return pltpu.make_async_copy(scales.at[rows, :], scale_ref.at[rows, :], out_sems.at[half_n * blocks + i])

    @pl.loop(0, blocks)
    def _(i):
        swap_sq(i).wait()
        rows = pl.ds(pl.multiple_of(i * ROWS, ROWS), ROWS)
        squares = jnp.sum(sq_send[rows, :] + sq_recv[rows, :], axis=1, keepdims=True)
        scales[rows, :] = jnp.broadcast_to(lax.rsqrt(squares / (2 * half) + epsilon), (ROWS, 128))
        write_scale(i).start()

    @pl.loop(n - 3, n - 1)
    def _(s):
        for k in range(len(views)):
            cw(k, s).wait_send()
            ccw(k, s).wait_send()
            if shared(k):
                across(k, s, rep).wait_send()

    @pl.loop(0, blocks)
    def _(i):
        for j in range(half_n):
            back_swap(j, i).wait_send()
            write(j, i).wait()
        write_scale(i).wait()


CHUNKS = 8


def closing_kernel(total_in, scale_in, out_ref, total, scale, result, sems):
    rows = total.shape[0] // CHUNKS

    def copies(i):
        at = pl.ds(i * rows, rows)
        return (
            pltpu.make_async_copy(total_in.at[at, :], total.at[at, :], sems.at[0, i]),
            pltpu.make_async_copy(scale_in.at[at, :], scale.at[at, :], sems.at[1, i]),
            pltpu.make_async_copy(result.at[at, :], out_ref.at[at, :], sems.at[2, i]),
        )

    for i in range(CHUNKS):
        first, second, _ = copies(i)
        first.start()
        second.start()
    for i in range(CHUNKS):
        first, second, third = copies(i)
        first.wait()
        second.wait()
        at = pl.ds(i * rows, rows)
        result[at, :] = (total[at, :].astype(F32) * scale[at, :1]).astype(BF16)
        third.start()
    for i in range(CHUNKS):
        copies(i)[2].wait()


def fused(n, stream_in, decay_shift, mixer_gain, gate_weight, input_weight, filter_taps, recur_gate,
          inlet_gate, decay_param, mixer_out, feedforward_gain, up_weight, down_weight, final_gain):
    _, length, half = stream_in.shape
    shard, channels = gate_weight.shape
    hidden = up_weight.shape[1]
    width = down_weight.shape[1]
    model = shard * n
    blocks = length // ROWS
    half_n = n // 2
    vmem = pl.BlockSpec(memory_space=pltpu.VMEM)
    hbm = pl.BlockSpec(memory_space=pl.ANY)
    swaps = 1 + 2 * blocks + half_n * blocks + blocks
    total, scale = pl.pallas_call(
        functools.partial(layer_kernel, n),
        out_shape=(jax.ShapeDtypeStruct((length, half), BF16), jax.ShapeDtypeStruct((length, 128), F32)),
        in_specs=[hbm] * 14,
        out_specs=(hbm, hbm),
        scratch_shapes=[
            pltpu.VMEM((1, length), F32),
            pltpu.VMEM((1, model), F32),
            pltpu.VMEM(filter_taps.shape, F32),
            pltpu.VMEM(recur_gate.shape, BF16),
            pltpu.VMEM(inlet_gate.shape, BF16),
            pltpu.VMEM((1, channels), F32),
            pltpu.VMEM((1, model), F32),
            pltpu.VMEM((1, half), F32),
            pltpu.VMEM((length, half), BF16),
            pltpu.VMEM((model, channels), BF16),
            pltpu.VMEM((model, channels), BF16),
            pltpu.VMEM((n, channels, width), BF16),
            pltpu.VMEM((model, hidden), BF16),
            pltpu.VMEM((n, hidden, width), BF16),
            pltpu.VMEM((length, half), BF16),
            pltpu.VMEM((length, model), BF16),
            pltpu.VMEM((8 + ROWS, channels), F32),
            pltpu.VMEM((8, channels), F32),
            pltpu.VMEM((ROWS, channels), F32),
            pltpu.VMEM((ROWS, channels), F32),
            pltpu.VMEM((2, length, half), BF16),
            pltpu.VMEM((length, half), BF16),
            pltpu.VMEM((length, half), BF16),
            pltpu.VMEM((length, half), BF16),
            pltpu.VMEM((length, hidden), BF16),
            pltpu.VMEM((length, 128), F32),
            pltpu.VMEM((length, 128), F32),
            pltpu.VMEM((2, length, width), F32),
            pltpu.VMEM((length, 128), F32),
            pltpu.SemaphoreType.DMA((14,)),
            pltpu.SemaphoreType.DMA((9, 3, 2)),
            pltpu.SemaphoreType.DMA((9, 3, n - 1)),
            pltpu.SemaphoreType.DMA((swaps,)),
            pltpu.SemaphoreType.DMA((swaps,)),
            pltpu.SemaphoreType.DMA((half_n * blocks + blocks,)),
        ],
        compiler_params=pltpu.CompilerParams(
            collective_id=0, has_side_effects=True, vmem_limit_bytes=67043328
        ),
        name="gated_layer",
    )(
        stream_in.reshape(length, half),
        decay_shift,
        mixer_gain.reshape(1, -1),
        gate_weight,
        input_weight,
        filter_taps,
        recur_gate,
        inlet_gate,
        decay_param.reshape(1, -1),
        mixer_out,
        feedforward_gain.reshape(1, -1),
        up_weight,
        down_weight,
        final_gain.reshape(1, -1),
    )
    out = pl.pallas_call(
        closing_kernel,
        out_shape=jax.ShapeDtypeStruct((length, half), BF16),
        in_specs=[hbm, hbm],
        out_specs=hbm,
        scratch_shapes=[
            pltpu.VMEM((length, half), BF16),
            pltpu.VMEM((length, 128), F32),
            pltpu.VMEM((length, half), BF16),
            pltpu.SemaphoreType.DMA((3, CHUNKS)),
        ],
        name="closing",
    )(total, scale)
    return out.reshape(1, length, half)


def fits(mesh, n, args):
    num_seq, length, half = args[0].shape
    width = args[9].shape[1]
    shard = args[3].shape[0]
    return (
        mesh.shape["rep"] == 2 and mesh.shape["tp"] == 2 and n % 8 == 0 and num_seq == 1
        and width % 128 == 0 and args[11].shape[1] % 1024 == 0 and length == 4 * ROWS and shard >= 3 * TILE and length % ROWS == 0
    )


def local_for(mesh):
    n = mesh.shape["fs"]

    def local(*args):
        if fits(mesh, n, args):
            return fused(n, *args)
        return plain(*args)

    return local


def solution(mesh):
    return jax.shard_map(
        local_for(mesh),
        mesh=mesh,
        in_specs=(
            P(("rep", "fs"), None, "tp"),
            P(("rep", "fs"), None),
            P(),
            P("fs", "tp"),
            P("fs", "tp"),
            P(None, "tp"),
            P("tp", None, None),
            P("tp", None, None),
            P("tp"),
            P("tp", "fs"),
            P(),
            P("fs", "tp"),
            P("tp", "fs"),
            P("tp"),
        ),
        out_specs=P(("rep", "fs"), None, "tp"),
        check_vma=False,
    )
```

```python
import functools

import jax
import jax.numpy as jnp
from jax import lax
from jax.experimental import pallas as pl
from jax.experimental.pallas import tpu as pltpu
from jax.sharding import PartitionSpec as P

D = 2048


epsilon = 1e-06
rate_scale = 8.0


def norm_rows(values, row_gain):
    mean_sq = jnp.mean(values * values, axis=-1, keepdims=True)
    return values * lax.rsqrt(mean_sq + epsilon) * row_gain


def combine(earlier, later):
    return (earlier[0] * later[0], later[0] * earlier[1] + later[1])


def plain(
    stream_in,
    decay_shift,
    mixer_gain,
    gate_weight,
    input_weight,
    filter_taps,
    recur_gate,
    inlet_gate,
    decay_param,
    mixer_out,
    feedforward_gain,
    up_weight,
    down_weight,
    final_gain,
):
    num_seq, length, half_width = stream_in.shape
    whole = lax.all_gather(stream_in, "tp", axis=2, tiled=True)
    flat_rows = num_seq * length
    normed = norm_rows(whole.reshape(flat_rows, -1).astype(jnp.float32), mixer_gain).astype(
        jnp.bfloat16
    )
    channels = gate_weight.shape[1]
    columns = normed
    gate_logits = jnp.dot(
        columns,
        lax.all_gather(gate_weight, "fs", axis=0, tiled=True),
        preferred_element_type=jnp.float32,
    )
    input_pre = jnp.dot(
        columns,
        lax.all_gather(input_weight, "fs", axis=0, tiled=True),
        preferred_element_type=jnp.float32,
    )
    gate_logits = gate_logits.astype(jnp.bfloat16)
    input_pre = input_pre.astype(jnp.bfloat16)
    branch = jax.nn.gelu(gate_logits.astype(jnp.float32), approximate=True)
    num_taps = filter_taps.shape[0]
    extended_front = jnp.pad(
        input_pre.astype(jnp.float32).reshape(num_seq, length, channels),
        ((0, 0), (num_taps - 1, 0), (0, 0)),
    )
    filtered = jnp.zeros((num_seq, length, channels), jnp.float32)
    for offset in range(num_taps):
        filtered = (
            filtered
            + extended_front[:, offset : offset + length] * filter_taps[offset][None, None, :]
        )
    filtered = filtered.astype(jnp.bfloat16).reshape(flat_rows, channels)
    num_blocks = recur_gate.shape[0]
    grouped = filtered.reshape(flat_rows, num_blocks, recur_gate.shape[1])
    recur = jax.nn.sigmoid(
        jnp.einsum("lni,nij->lnj", grouped, recur_gate, preferred_element_type=jnp.float32).reshape(
            flat_rows, channels
        )
    )
    inlet = jax.nn.sigmoid(
        jnp.einsum("lni,nij->lnj", grouped, inlet_gate, preferred_element_type=jnp.float32).reshape(
            flat_rows, channels
        )
    )
    logarithm_decay = (
        -rate_scale * recur * jax.nn.softplus(-decay_param)[None, :]
        + decay_shift.reshape(flat_rows)[:, None]
    )
    decay = jnp.exp(logarithm_decay).reshape(num_seq, length, channels)
    drive = (
        jnp.sqrt(-jnp.expm1(2.0 * logarithm_decay)) * inlet * filtered.astype(jnp.float32)
    ).reshape(num_seq, length, channels)
    states = lax.associative_scan(combine, (decay, drive), axis=1)[1]
    mixed = (states.reshape(flat_rows, channels) * branch).astype(jnp.bfloat16)
    mixer_terms = (
        jnp.dot(
            mixed,
            lax.all_gather(mixer_out, "fs", axis=1, tiled=True),
            preferred_element_type=jnp.float32,
        )
        .astype(jnp.bfloat16)
        .astype(jnp.float32)
    )
    mixer_sum = lax.psum_scatter(
        mixer_terms.astype(jnp.bfloat16), "tp", scatter_dimension=1, tiled=True
    ).astype(jnp.float32)
    stream_mid = (stream_in.reshape(flat_rows, half_width).astype(jnp.float32) + mixer_sum).astype(
        jnp.bfloat16
    )
    stream_whole = lax.all_gather(stream_mid, "tp", axis=1, tiled=True)
    normed_mid = norm_rows(stream_whole.astype(jnp.float32), feedforward_gain).astype(jnp.bfloat16)
    columns = normed_mid
    up_proj = jnp.dot(
        columns,
        lax.all_gather(up_weight, "fs", axis=0, tiled=True),
        preferred_element_type=jnp.float32,
    )
    activated = jnp.square(jax.nn.relu(up_proj)).astype(jnp.bfloat16)
    ffn_terms = (
        jnp.dot(
            activated,
            lax.all_gather(down_weight, "fs", axis=1, tiled=True),
            preferred_element_type=jnp.float32,
        )
        .astype(jnp.bfloat16)
        .astype(jnp.float32)
    )
    ffn_sum = lax.psum_scatter(
        ffn_terms.astype(jnp.bfloat16), "tp", scatter_dimension=1, tiled=True
    ).astype(jnp.float32)
    total = stream_mid.astype(jnp.float32) + ffn_sum
    squares_sum = lax.psum(jnp.sum(total * total, axis=1), "tp")
    layer_out = total * lax.rsqrt(squares_sum / D + epsilon)[:, None] * final_gain[None, :]
    return layer_out.astype(jnp.bfloat16).reshape(num_seq, length, half_width)


F32 = jnp.float32
BF16 = jnp.bfloat16
TILE = 16
FORE, BACK, BOTH = range(3)
ROWS = 256


def split_rows(rows, up):
    third = rows // 3 // TILE * TILE + (TILE if up else 0)
    return rows - 2 * third, third


def expm1_neg(v):
    series = -v * (1.0 + v * (1 / 2) * (1.0 + v * (1 / 3) * (1.0 + v * (1 / 4) * (1.0 + v * (1 / 5) * (1.0 + v * (1 / 6))))))
    return jnp.where(v > -0.25, series, 1.0 - jnp.exp(v))


def layer_kernel(
    n,
    x_in, shift_in, mgain_in, wg_in, wi_in, taps_in, rg_in, ig_in, sp_in, wo_in,
    fgain_in, wu_in, wd_in, lgain_in,
    out_ref, scale_ref,
    shift_ref, mgain_ref, taps_ref, rg_ref, ig_ref, sp_ref, fgain_ref, lgain_ref,
    x_ref, wg, wi, wo, wu, wd, other, normed, front, carry, scan_a, scan_b, part, prec, mid, mid_other,
    act, sq_send, sq_recv, acc, scales,
    local_sems, send_sems, recv_sems, across_sems, tp_send, tp_recv, out_sems,
):
    rep, fs, tp = lax.axis_index("rep"), lax.axis_index("fs"), lax.axis_index("tp")
    half_n = n // 2
    length, half = x_in.shape
    channels = wg.shape[1]
    width = wd.shape[2]
    shard = wg_in.shape[0]
    hidden = wu.shape[1]
    blocks = length // ROWS

    def ring_to_fs(p):
        p = lax.rem(p + 2 * n, n)
        return jnp.where(p < half_n, 2 * p, 2 * (n - 1 - p) + 1)

    odd = lax.rem(fs, 2)
    pos = (1 - odd) * (fs // 2) + odd * (n - 1 - fs // 2)
    right, left = ring_to_fs(pos + 1), ring_to_fs(pos - 1)

    def by_row(dst, lo, cols):
        def view(owner, off, size):
            return dst.at[pl.ds(pl.multiple_of(owner * shard + off, TILE), size), pl.ds(lo, cols)]
        return view

    def by_owner(dst, lo):
        def view(owner, off, size):
            return dst.at[owner, pl.ds(pl.multiple_of(lo + off, TILE), size), :]
        return view

    rows_o, rows_d = wo.shape[1], wd.shape[1]
    def plain_split(rows, up):
        p, q = split_rows(rows, up)
        return (0, p), (p, q)

    quarter = hidden // 4
    half_d = rows_d // 2
    private, last = rows_d // 8, rows_d // 16
    common = half_d - 2 * private - last
    views = [
        (by_row(wg, 0, channels), BACK, plain_split(shard, True)),
        (by_row(wi, 0, channels), FORE, plain_split(shard, True)),
        (by_owner(wo, 0), FORE, plain_split(rows_o, True)),
        (by_row(wu, 0, quarter), BACK, plain_split(shard, True)),
        (by_row(wu, quarter, 2 * quarter), FORE, plain_split(shard, True)),
        (by_row(wu, 3 * quarter, quarter), BACK, plain_split(shard, True)),
        (by_owner(wd, 0), FORE, ((0, common), (half_d, private))),
        (by_owner(wd, 0), BACK, ((half_d + 2 * private, common), (common + last, private))),
        (by_owner(wd, 0), BOTH, ((common, last), (rows_d - last, last))),
    ]
    ups = range(3, 6)
    downs = range(6, 9)

    def remote(view, k, lane, s, device):
        return pltpu.make_async_remote_copy(
            src_ref=view, dst_ref=view, send_sem=send_sems.at[k, lane, lax.rem(s, 2)],
            recv_sem=across_sems.at[k, s] if lane == 2 else recv_sems.at[k, lane, lax.rem(s, 4)], device_id=device,
            device_id_type=pl.DeviceIdType.MESH,
        )

    def cw(k, s, shift=0):
        view, role, (whole, (lo, size)) = views[k]
        at = (lo + rep * size, size) if role == BACK else whole
        return remote(view(ring_to_fs(pos - s - shift), *at), k, 0, s, {"fs": right})

    def ccw(k, s, shift=0):
        view, role, (whole, (lo, size)) = views[k]
        at = whole if role == BACK else (lo + rep * size if role == FORE else lo, size)
        return remote(view(ring_to_fs(pos + s + shift), *at), k, 1, s, {"fs": left})

    def across(k, s, side):
        view, role, (_, (lo, size)) = views[k]
        owner = pos + s + 1 if role == FORE else pos - s - 1
        return remote(view(ring_to_fs(owner), lo + side * size, size), k, 2, s, {"rep": 1 - rep})

    def shared(k):
        return views[k][1] != BOTH

    def begin(k):
        cw(k, 0).start()
        ccw(k, 0).start()

    def launch(make, k, s, *side):
        pl.when(s >= 2)(lambda: make(k, s - 2, *side).wait_send())
        make(k, s, *side).start()

    def service(turns, s, last):
        for make, k in turns:
            make(k, s, 1).wait_recv()
            if last is None:
                pl.when(s + 1 < n - 1)(functools.partial(launch, make, k, s + 1))
            elif not last:
                launch(make, k, s + 1)
            if views[k][1] == (BACK if make is cw else FORE):
                launch(across, k, s, rep)

    def turns_of(back, fore, third):
        return [[(cw, back), (ccw, fore)], [(cw, fore), (ccw, back)], [(cw, third), (ccw, third)]]

    mixer_turns, up_turns, down_turns = turns_of(0, 1, 2), turns_of(3, 4, 5), turns_of(7, 6, 8)

    def wait_across(k, s):
        if shared(k):
            across(k, s, 1 - rep).wait_recv()

    def swap(src, dst, index):
        return pltpu.make_async_remote_copy(
            src_ref=src, dst_ref=dst, send_sem=tp_send.at[index], recv_sem=tp_recv.at[index],
            device_id={"tp": 1 - tp}, device_id_type=pl.DeviceIdType.MESH,
        )

    own = [
        (x_in, x_ref),
        (wg_in, wg.at[pl.ds(pl.multiple_of(fs * shard, TILE), shard), :]),
        (wi_in, wi.at[pl.ds(pl.multiple_of(fs * shard, TILE), shard), :]),
        (wo_in, wo.at[fs]),
        (wu_in, wu.at[pl.ds(pl.multiple_of(fs * shard, TILE), shard), :]),
        (wd_in, wd.at[fs]),
        (mgain_in, mgain_ref),
        (shift_in, shift_ref),
        (taps_in, taps_ref),
        (rg_in, rg_ref),
        (ig_in, ig_ref),
        (sp_in, sp_ref),
        (fgain_in, fgain_ref),
        (lgain_in, lgain_ref),
    ]
    local = [pltpu.make_async_copy(a, b, local_sems.at[i]) for i, (a, b) in enumerate(own)]
    barrier = pltpu.get_barrier_semaphore()
    for device in ({"fs": right}, {"fs": left}, {"rep": 1 - rep}, {"tp": 1 - tp}):
        pl.semaphore_signal(barrier, inc=1, device_id=device, device_id_type=pl.DeviceIdType.MESH)
    for i in (1, 2, 3, 0, 4, 5, *range(6, len(own))):
        local[i].start()
    pl.semaphore_wait(barrier, 4)
    swap_x = swap(x_ref, other, 0)
    for k in range(3):
        local[1 + k].wait()
    for turns in mixer_turns:
        for make, k in turns:
            make(k, 0).start()
    local[0].wait()
    swap_x.start()
    for i in range(4, len(own)):
        local[i].wait()

    own_cols = pl.ds(pl.multiple_of(tp * half, 128), half)
    other_cols = pl.ds(pl.multiple_of((1 - tp) * half, 128), half)

    def norm_block(first, second, gain_ref, rows):
        a = first[rows, :].astype(F32)
        b = second[rows, :].astype(F32)
        mean = (jnp.sum(a * a, axis=1, keepdims=True) + jnp.sum(b * b, axis=1, keepdims=True)) / (2 * half)
        scale = lax.rsqrt(mean + epsilon)
        normed[rows, own_cols] = (a * scale * gain_ref[:, own_cols]).astype(BF16)
        normed[rows, other_cols] = (b * scale * gain_ref[:, other_cols]).astype(BF16)

    small = 64

    pieces = length // small
    share = -(-pieces // (n - 2))

    @pl.loop(0, n - 2)
    def _(s):
        for turns in mixer_turns:
            service(turns, s, False)
        pl.when(s == 0)(swap_x.wait)

        @pl.when(s == n - 4)
        def _():
            for make, k in up_turns[0] + up_turns[1]:
                make(k, 0).start()

        for piece in range(share):
            i = s * share + piece

            @pl.when(i < pieces)
            def _():
                norm_block(x_ref, other, mgain_ref, pl.ds(pl.multiple_of(i * small, small), small))

    begin(ups[-1])
    for turns in mixer_turns:
        service(turns, n - 2, True)

    lead = n - 2

    def tick(t, j):
        pl.when(t < n - 1)(lambda: service(up_turns[j], t, None))

        if j == 2:

            @pl.when(t == n - 5)
            def _():
                for make, k in down_turns[0]:
                    make(k, 0).start()

            @pl.when(t == n - 4)
            def _():
                for make, k in down_turns[1]:
                    make(k, 0).start()
                begin(downs[2])

        pl.when(t >= lead)(lambda: service(down_turns[j], t - lead, None))

    for j in range(3):
        tick(0, j)

    @pl.loop(0, n - 1)
    def _(s):
        for k in range(3):
            wait_across(k, s)

    front[pl.ds(0, 8), :] = jnp.zeros((8, channels), F32)
    carry[...] = jnp.zeros_like(carry)
    decay_param = sp_ref[...]
    rate = rate_scale * (jnp.maximum(-decay_param, 0.0) + jnp.log1p(jnp.exp(-jnp.abs(decay_param))))
    num_taps = taps_ref.shape[0]
    groups = rg_ref.shape[0]
    block = rg_ref.shape[1]
    @pl.loop(0, blocks)
    def _(i):
        rows = pl.ds(pl.multiple_of(i * ROWS, ROWS), ROWS)
        tick(i + 1, 0)
        cols = normed[rows, :]
        front[pl.ds(8, ROWS), :] = jnp.dot(cols, wi[...], preferred_element_type=F32).astype(BF16).astype(F32)
        gate = jnp.dot(cols, wg[...], preferred_element_type=F32).astype(BF16)
        shift = jnp.transpose(jnp.broadcast_to(shift_ref[:, rows], (128, ROWS)))[:, :1]
        for g in range(groups):
            if g == 1:
                tick(i + 1, 1)
            ch = slice(g * block, (g + 1) * block)
            window = front[:, ch]
            filtered = jnp.zeros((ROWS, block), F32)
            for tap in range(num_taps):
                back = num_taps - 1 - tap
                moved = window if back == 0 else pltpu.roll(window, back, 0)
                filtered = filtered + moved[8:] * taps_ref[tap : tap + 1, ch]
            filtered = filtered.astype(BF16)
            recur = jax.nn.sigmoid(jnp.dot(filtered, rg_ref[g], preferred_element_type=F32))
            inlet = jax.nn.sigmoid(jnp.dot(filtered, ig_ref[g], preferred_element_type=F32))
            log_decay = shift - recur * rate[:, ch]
            a = jnp.exp(log_decay)
            b = jnp.sqrt(expm1_neg(2.0 * log_decay)) * inlet * filtered.astype(F32)
            a = a.reshape(ROWS // 8, 8, block)
            b = b.reshape(ROWS // 8, 8, block)
            at = lax.broadcasted_iota(jnp.int32, (ROWS // 8, 8, block), 1)
            for back in (1, 2, 4):
                keep = at >= back
                b = jnp.where(keep, a * pltpu.roll(b, back, 1) + b, b)
                a = jnp.where(keep, a * pltpu.roll(a, back, 1), a)
            scan_a[:, ch] = a.reshape(ROWS, block)
            scan_b[:, ch] = b.reshape(ROWS, block)
        front[pl.ds(0, 8), :] = front[pl.ds(ROWS, 8), :]

        def step_scan(t, h):
            at = pl.ds(pl.multiple_of(t * 8, 8), 8)
            states = scan_a[at, :] * h + scan_b[at, :]
            scan_b[at, :] = states
            return jnp.broadcast_to(states[7:8, :], states.shape)

        carry[...] = lax.fori_loop(0, ROWS // 8, step_scan, carry[...], unroll=4)
        tick(i + 1, 2)
        mixed = (scan_b[...] * jax.nn.gelu(gate.astype(F32), approximate=True)).astype(BF16)
        for j in range(half_n):
            to = pl.ds(j * width, width)
            part[1, rows, to] = jnp.dot(mixed, wo[(1 - tp) * half_n + j], preferred_element_type=F32).astype(BF16)
        swap(part.at[1, rows, :], prec.at[rows, :], 1 + i).start()
        for j in range(half_n):
            to = pl.ds(j * width, width)
            part[0, rows, to] = jnp.dot(mixed, wo[tp * half_n + j], preferred_element_type=F32).astype(BF16)

    tick(blocks + 1, 0)

    @pl.loop(0, blocks)
    def _(i):
        rows = pl.ds(pl.multiple_of(i * ROWS, ROWS), ROWS)
        swap(part.at[1, rows, :], prec.at[rows, :], 1 + i).wait()
        mid[rows, :] = (
            x_ref[rows, :].astype(F32) + (part[0, rows, :].astype(F32) + prec[rows, :].astype(F32))
        ).astype(BF16)
        swap(mid.at[rows, :], mid_other.at[rows, :], 1 + blocks + i).start()

    tick(blocks + 1, 1)

    @pl.loop(0, blocks)
    def _(i):
        rows = pl.ds(pl.multiple_of(i * ROWS, ROWS), ROWS)
        swap(mid.at[rows, :], mid_other.at[rows, :], 1 + blocks + i).wait()

    tick(blocks + 1, 2)

    for part_of in range(2):

        @pl.loop(part_of * (pieces // 2), (part_of + 1) * (pieces // 2))
        def _(i):
            norm_block(mid, mid_other, fgain_ref, pl.ds(pl.multiple_of(i * small, small), small))

        tick(blocks + 2, part_of)

    tick(blocks + 2, 2)
    for t in range(blocks + 3, n + 1):
        for j in range(3):
            tick(t, j)

    @pl.loop(0, n - 1)
    def _(s):
        for k in ups:
            wait_across(k, s)

    up_cols = min(512, hidden)
    @pl.loop(0, hidden // up_cols)
    def _(c):
        to = pl.ds(pl.multiple_of(c * up_cols, up_cols), up_cols)

        @pl.loop(0, blocks)
        def _(i):
            rows = pl.ds(pl.multiple_of(i * ROWS, ROWS), ROWS)
            up = jnp.maximum(jnp.dot(normed[rows, :], wu[:, to], preferred_element_type=F32), 0.0)
            act[rows, to] = (up * up).astype(BF16)

        for j in range(3):
            pl.when(c == j)(functools.partial(tick, n + 1, j))

    tick(n + 2, 0)

    def place(owner, i):
        column = lax.rem(owner, half_n)
        slot = lax.rem(owner // half_n + tp, 2)
        rows = pl.ds(pl.multiple_of(i * ROWS, ROWS), ROWS)
        to = pl.ds(pl.multiple_of(column * width, 128), width)
        return column, slot, rows, to

    def back_swap(column, i):
        _, _, rows, to = place(column, i)
        return swap(part.at[1, rows, to], prec.at[rows, to], 1 + 2 * blocks + column * blocks + i)

    def write(column, i):
        _, _, rows, to = place(column, i)
        return pltpu.make_async_copy(other.at[rows, to], out_ref.at[rows, to], out_sems.at[column])

    def down_rows(owner, i):
        column, slot, rows, to = place(owner, i)
        part[slot, rows, to] = jnp.dot(act[rows, :], wd[owner], preferred_element_type=F32).astype(BF16)
        pl.when(slot == 1)(lambda: back_swap(column, i).start())

    def early_rows(e, owner, i):
        rows = pl.ds(pl.multiple_of(i * ROWS, ROWS), ROWS)
        take = pl.ds((1 - e) * half_d, half_d)
        acc[e, rows, :] = jnp.dot(act[rows, take], wd[owner, take, :], preferred_element_type=F32)

    def late_rows(e, owner, i):
        column, slot, rows, to = place(owner, i)
        take = pl.ds(e * half_d, half_d)
        rest = jnp.dot(act[rows, take], wd[owner, take, :], preferred_element_type=F32)
        part[slot, rows, to] = (acc[e, rows, :] + rest).astype(BF16)
        pl.when(slot == 1)(lambda: back_swap(column, i).start())

    def total_rows(owner, i):
        column, slot, rows, to = place(owner, i)

        @pl.when(slot == 0)
        def _():
            back_swap(column, i).wait_recv()
            total = mid[rows, to].astype(F32) + (part[0, rows, to].astype(F32) + prec[rows, to].astype(F32))
            other[rows, to] = (total * lgain_ref[:, to]).astype(BF16)
            squares = total * total
            sq_send[rows, :] += sum(squares[:, at : at + 128] for at in range(0, width, 128))
            write(column, i).start()

    def over_rows(*makes):
        @pl.loop(0, blocks)
        def _(i):
            for make, owner in makes:
                make(owner, i)

    order = [ring_to_fs(pos + ahead) for ahead in [0, half_n]]
    for s in range(half_n, n - 1):
        order += [ring_to_fs(pos - s - 1), ring_to_fs(pos + s + 1)]
    sq_send[...] = jnp.zeros_like(sq_send)
    over_rows((down_rows, order[0]))
    for at in range(3 * n + 7, 3 * (lead + half_n + 1)):
        tick(at // 3, at % 3)
    for s in range(half_n):
        for k in downs:
            wait_across(k, s)
    over_rows((down_rows, order[1]), (total_rows, order[0]))
    for e in range(2):
        over_rows((functools.partial(early_rows, e), order[e - 2]))
    for s in range(half_n, n - 2):
        at = 2 * (s - half_n + 1)
        tick(lead + s + 1, 0)
        for k in downs:
            wait_across(k, s)
        over_rows((down_rows, order[at]), (total_rows, order[at - 1]))
        tick(lead + s + 1, 1)
        over_rows((down_rows, order[at + 1]), (total_rows, order[at]))
        tick(lead + s + 1, 2)
    wait_across(downs[1], n - 2)
    over_rows((functools.partial(late_rows, 0), order[-2]), (total_rows, order[-3]))
    wait_across(downs[0], n - 2)

    def swap_sq(i):
        rows = pl.ds(pl.multiple_of(i * ROWS, ROWS), ROWS)
        return swap(sq_send.at[rows, :], sq_recv.at[rows, :], 1 + 2 * blocks + half_n * blocks + i)

    def settle(i):
        total_rows(order[-2], i)
        total_rows(order[-1], i)
        swap_sq(i).start()

    @pl.loop(0, blocks)
    def _(i):
        late_rows(1, order[-1], i)
        pl.when(i > 0)(lambda: settle(i - 1))

    settle(blocks - 1)

    def write_scale(i):
        rows = pl.ds(pl.multiple_of(i * ROWS, ROWS), ROWS)
        return pltpu.make_async_copy(scales.at[rows, :], scale_ref.at[rows, :], out_sems.at[half_n])

    @pl.loop(0, blocks)
    def _(i):
        swap_sq(i).wait()
        rows = pl.ds(pl.multiple_of(i * ROWS, ROWS), ROWS)
        squares = jnp.sum(sq_send[rows, :] + sq_recv[rows, :], axis=1, keepdims=True)
        scales[rows, :] = jnp.broadcast_to(lax.rsqrt(squares / (2 * half) + epsilon), (ROWS, 128))
        write_scale(i).start()

    @pl.loop(n - 3, n - 1)
    def _(s):
        for k in range(len(views)):
            cw(k, s).wait_send()
            ccw(k, s).wait_send()
            if shared(k):
                across(k, s, rep).wait_send()

    for j in range(half_n):
        to = pl.ds(j * width, width)
        pltpu.make_async_copy(other.at[:, to], out_ref.at[:, to], out_sems.at[j]).wait()
    pltpu.make_async_copy(scales, scale_ref, out_sems.at[half_n]).wait()

    @pl.loop(0, blocks)
    def _(i):
        for j in range(half_n):
            back_swap(j, i).wait_send()


CHUNKS = 8


def closing_kernel(total_in, scale_in, out_ref, total, scale, result, sems):
    rows = total.shape[0] // CHUNKS

    def copies(i):
        at = pl.ds(i * rows, rows)
        return (
            pltpu.make_async_copy(total_in.at[at, :], total.at[at, :], sems.at[0, i]),
            pltpu.make_async_copy(scale_in.at[at, :], scale.at[at, :], sems.at[1, i]),
            pltpu.make_async_copy(result.at[at, :], out_ref.at[at, :], sems.at[2, i]),
        )

    for i in range(CHUNKS):
        first, second, _ = copies(i)
        first.start()
        second.start()
    for i in range(CHUNKS):
        first, second, third = copies(i)
        first.wait()
        second.wait()
        at = pl.ds(i * rows, rows)
        result[at, :] = (total[at, :].astype(F32) * scale[at, :1]).astype(BF16)
        third.start()
    for i in range(CHUNKS):
        copies(i)[2].wait()


def fused(n, stream_in, decay_shift, mixer_gain, gate_weight, input_weight, filter_taps, recur_gate,
          inlet_gate, decay_param, mixer_out, feedforward_gain, up_weight, down_weight, final_gain):
    _, length, half = stream_in.shape
    shard, channels = gate_weight.shape
    hidden = up_weight.shape[1]
    width = down_weight.shape[1]
    model = shard * n
    blocks = length // ROWS
    half_n = n // 2
    vmem = pl.BlockSpec(memory_space=pltpu.VMEM)
    hbm = pl.BlockSpec(memory_space=pl.ANY)
    swaps = 1 + 2 * blocks + half_n * blocks + blocks
    total, scale = pl.pallas_call(
        functools.partial(layer_kernel, n),
        out_shape=(jax.ShapeDtypeStruct((length, half), BF16), jax.ShapeDtypeStruct((length, 128), F32)),
        in_specs=[hbm] * 14,
        out_specs=(hbm, hbm),
        scratch_shapes=[
            pltpu.VMEM((1, length), F32),
            pltpu.VMEM((1, model), F32),
            pltpu.VMEM(filter_taps.shape, F32),
            pltpu.VMEM(recur_gate.shape, BF16),
            pltpu.VMEM(inlet_gate.shape, BF16),
            pltpu.VMEM((1, channels), F32),
            pltpu.VMEM((1, model), F32),
            pltpu.VMEM((1, half), F32),
            pltpu.VMEM((length, half), BF16),
            pltpu.VMEM((model, channels), BF16),
            pltpu.VMEM((model, channels), BF16),
            pltpu.VMEM((n, channels, width), BF16),
            pltpu.VMEM((model, hidden), BF16),
            pltpu.VMEM((n, hidden, width), BF16),
            pltpu.VMEM((length, half), BF16),
            pltpu.VMEM((length, model), BF16),
            pltpu.VMEM((8 + ROWS, channels), F32),
            pltpu.VMEM((8, channels), F32),
            pltpu.VMEM((ROWS, channels), F32),
            pltpu.VMEM((ROWS, channels), F32),
            pltpu.VMEM((2, length, half), BF16),
            pltpu.VMEM((length, half), BF16),
            pltpu.VMEM((length, half), BF16),
            pltpu.VMEM((length, half), BF16),
            pltpu.VMEM((length, hidden), BF16),
            pltpu.VMEM((length, 128), F32),
            pltpu.VMEM((length, 128), F32),
            pltpu.VMEM((2, length, width), F32),
            pltpu.VMEM((length, 128), F32),
            pltpu.SemaphoreType.DMA((14,)),
            pltpu.SemaphoreType.DMA((9, 3, 2)),
            pltpu.SemaphoreType.DMA((9, 2, 4)),
            pltpu.SemaphoreType.DMA((8, n - 1)),
            pltpu.SemaphoreType.DMA((swaps,)),
            pltpu.SemaphoreType.DMA((swaps,)),
            pltpu.SemaphoreType.DMA((half_n + 1,)),
        ],
        compiler_params=pltpu.CompilerParams(
            collective_id=0, has_side_effects=True, vmem_limit_bytes=67043328
        ),
        name="gated_layer",
    )(
        stream_in.reshape(length, half),
        decay_shift,
        mixer_gain.reshape(1, -1),
        gate_weight,
        input_weight,
        filter_taps,
        recur_gate,
        inlet_gate,
        decay_param.reshape(1, -1),
        mixer_out,
        feedforward_gain.reshape(1, -1),
        up_weight,
        down_weight,
        final_gain.reshape(1, -1),
    )
    out = pl.pallas_call(
        closing_kernel,
        out_shape=jax.ShapeDtypeStruct((length, half), BF16),
        in_specs=[hbm, hbm],
        out_specs=hbm,
        scratch_shapes=[
            pltpu.VMEM((length, half), BF16),
            pltpu.VMEM((length, 128), F32),
            pltpu.VMEM((length, half), BF16),
            pltpu.SemaphoreType.DMA((3, CHUNKS)),
        ],
        name="closing",
    )(total, scale)
    return out.reshape(1, length, half)


def fits(mesh, n, args):
    num_seq, length, half = args[0].shape
    width = args[9].shape[1]
    shard = args[3].shape[0]
    return (
        mesh.shape["rep"] == 2 and mesh.shape["tp"] == 2 and n % 8 == 0 and num_seq == 1
        and width % 128 == 0 and args[11].shape[1] % 1024 == 0 and length == 4 * ROWS and shard >= 3 * TILE and length % ROWS == 0
    )


def local_for(mesh):
    n = mesh.shape["fs"]

    def local(*args):
        if fits(mesh, n, args):
            return fused(n, *args)
        return plain(*args)

    return local


def solution(mesh):
    return jax.shard_map(
        local_for(mesh),
        mesh=mesh,
        in_specs=(
            P(("rep", "fs"), None, "tp"),
            P(("rep", "fs"), None),
            P(),
            P("fs", "tp"),
            P("fs", "tp"),
            P(None, "tp"),
            P("tp", None, None),
            P("tp", None, None),
            P("tp"),
            P("tp", "fs"),
            P(),
            P("fs", "tp"),
            P("tp", "fs"),
            P("tp"),
        ),
        out_specs=P(("rep", "fs"), None, "tp"),
        check_vma=False,
    )
```
